32 devices in a mesh: fs: 8 (over z, x), tp: 4 (over y, core).
Axes of the slice: x: 2, y: 2, z: 4, core: 2. Of those that a mesh axis runs over, the one named last changes fastest.
Arguments:
- tokens: bfloat16 [1536, 2048], P('fs'), may hold values from -6 to 6
- norm_gain: float32 [2048], P('fs'), may hold values from 0.1 to 1.9
- expert_gate: float32 [16, 2048, 1024], P(None, 'fs', 'tp'), may hold values from -0.125 to 0.125
- expert_up: float32 [16, 2048, 1024], P(None, 'fs', 'tp'), may hold values from -0.125 to 0.125
- expert_down: float32 [16, 1024, 2048], P(None, 'fs', 'tp'), may hold values from -0.1875 to 0.1875
- shared_gate: float32 [2048, 1024], P('fs', 'tp'), may hold values from -0.125 to 0.125
- shared_up: float32 [2048, 1024], P('fs', 'tp'), may hold values from -0.125 to 0.125
- shared_down: float32 [1024, 2048], P('fs', 'tp'), may hold values from -0.1875 to 0.1875
- expert_ids: int32 [1536, 8], P('fs'), may hold values from 0 to 15, all different within a row; in each aligned block of 192 rows (0 to 191, 192 to 383, ...) at most 192 rows name the same one
- route_weights: float32 [1536, 8], P('fs'), may hold values from 0.25 to 1
Outputs:
- gate_ready: bfloat16 [16, 2048, 1024], P('fs', None, 'tp')
- up_ready: bfloat16 [16, 2048, 1024], P('fs', None, 'tp')
- down_ready: bfloat16 [16, 1024, 2048], P('fs', None, 'tp')
- shared_gate_ready: bfloat16 [2048, 1024], P(None, 'tp')
- shared_up_ready: bfloat16 [2048, 1024], P(None, 'tp')
- shared_down_ready: bfloat16 [1024, 2048], P(None, 'tp')
- mixed: bfloat16 [1536, 2048], P('fs', 'tp')
The draws below stay inside these ranges and needn't reach their ends.
Inputs may be any that keep to these rules, and one draw needn't show every extreme that they name: `expert_ids`: each row names 8 different experts. Among the 192 rows of one index of fs no expert is named more than 192 times, and in every draw some expert is named exactly 192 times there.
All inputs are finite; a program needn't handle non-finite values.
Results may differ from the reference program's by a relative error of at most 0.0085.
Values may be sent and summed in bfloat16 or wider, within the bound.
A program may use at most 128 MiB of HBM per device.

```python
import math
import jax
import jax.numpy as jnp
import numpy as np
from jax import lax

D = 2048
DE = 1024
TOP_K = 8
TOK_DEV = 192
EXPERTS = 16
TOKENS = 1536
CAPE = 192
N_FS = 8


def steps_of(own_key, extent, pieces, low, top_value):
    level, own = 1.0, jax.random.fold_in(own_key, 6)
    for axis_at, parts in pieces:
        draws = jnp.exp(jax.random.uniform(jax.random.fold_in(own, axis_at), (parts,), jnp.float32, low / len(pieces), top_value / len(pieces)))
        level = level * jnp.repeat(draws, extent[axis_at] // parts).reshape([-1 if axis == axis_at else 1 for axis in range(len(extent))])
    return level


def routed_block(key, own, number, rows, count, top, limit, slope):
    ranking = jax.random.permutation(key, count)
    crowded, common = shares(count, rows * top, limit, slope, True), shares(count, rows * top, limit, slope, False)
    places = jnp.arange(count)

    def named(tallies, offset_by):
        used = int((tallies > 0).sum())
        fixed = max(1, used // 4)
        moved = fixed + (places - fixed + offset_by * (used - fixed)) % max(1, count - fixed)
        return jnp.zeros((count,), jnp.int32).at[ranking[jnp.where(places < fixed, places, moved)]].set(jnp.asarray(tallies, jnp.int32))

    tallies = jnp.where(number % 4 == 0, named(crowded, number // 4), named(common, number - number // 4 - 1))
    mixed = jax.random.permutation(jax.random.fold_in(own, 3), count)
    giver, receiver = mixed[0:count // 2 * 2:2], mixed[1:count // 2 * 2:2]
    slack = jnp.minimum(tallies[giver] - 1, limit - tallies[receiver]) // 2
    slack = jnp.where((giver == ranking[0]) | (receiver == ranking[0]) | (tallies[receiver] == 0), 0, jnp.maximum(slack, 0))
    moved = jax.random.randint(jax.random.fold_in(own, 4), (count // 2,), 0, 1 << 20) % (slack + 1)
    tallies = tallies.at[giver].add(-moved).at[receiver].add(moved)
    members = jnp.searchsorted(jnp.cumsum(tallies), jnp.arange(rows * top), side="right").astype(jnp.int32)
    grid = members.reshape(top, rows).T
    grid = grid[jax.random.permutation(jax.random.fold_in(own, 1), rows)]
    offset_by = jax.random.randint(jax.random.fold_in(own, 2), (rows, 1), 0, top)
    return jnp.take_along_axis(grid, (jnp.arange(top)[None, :] + offset_by) % top, axis=1)


def shares(count, total, bound, lean, full):
    portions = [(1 << 20) // math.isqrt(rank ** lean) + 1 for rank in range(1, count + 1)]
    largest = bound if full else min(bound, max(-(-total // count), total * portions[0] // sum(portions)))
    least = 1 if total - largest >= count - 1 else 0
    counts, spare = [largest] + [least] * (count - 1), total - largest - least * (count - 1)
    while spare > 0:
        candidates = [i for i in range(1, count) if counts[i] < largest] or [i for i in range(1, count) if counts[i] < bound]
        pool, remaining = sum([portions[i] for i in candidates]), spare
        for i in candidates:
            more = min(bound - counts[i], max(1, remaining * portions[i] // pool), spare)
            counts[i] = counts[i] + more
            spare = spare - more
    return np.array(counts)


def scatter_about(own_key, dims, spread, reach, cuts=(), kind=jnp.bfloat16):
    values = spread * jax.random.normal(own_key, dims, jnp.float32)
    if cuts:
        values = values * steps_of(own_key, dims, cuts, -0.22, 0.18)
    return jnp.clip(values, -reach, reach).astype(kind)


def setup_inputs(seed: int = 0) -> dict:
    arg_keys = jax.random.split(jax.random.key(seed), 11)
    tokens = scatter_about(arg_keys[0], (TOKENS, D), 1.0, 6.0, ((0, 8),))
    norm_gain = jnp.clip(1.0 + 0.18 * jax.random.normal(arg_keys[1], (D,), jnp.float32), 0.1, 1.9)
    expert_gate = scatter_about(arg_keys[2], (EXPERTS, D, DE), D ** -0.5, 0.125, ((1, 8), (2, 4)), jnp.float32)
    expert_up = scatter_about(arg_keys[3], (EXPERTS, D, DE), D ** -0.5, 0.125, ((1, 8), (2, 4)), jnp.float32)
    expert_down = scatter_about(arg_keys[4], (EXPERTS, DE, D), DE ** -0.5, 0.1875, ((1, 8), (2, 4)), jnp.float32)
    shared_gate = scatter_about(arg_keys[5], (D, DE), D ** -0.5, 0.125, ((0, 8), (1, 4)), jnp.float32)
    shared_up = scatter_about(arg_keys[6], (D, DE), D ** -0.5, 0.125, ((0, 8), (1, 4)), jnp.float32)
    shared_down = scatter_about(arg_keys[7], (DE, D), DE ** -0.5, 0.1875, ((0, 8), (1, 4)), jnp.float32)
    expert_ids_keys = jax.random.split(jax.random.fold_in(arg_keys[8], 1), TOKENS // TOK_DEV)
    expert_ids_turns = jax.random.permutation(jax.random.fold_in(arg_keys[8], 3), TOKENS // TOK_DEV)
    expert_ids = jax.vmap(lambda own, number: routed_block(jax.random.fold_in(arg_keys[8], 2), own, number, TOK_DEV, EXPERTS, TOP_K, CAPE, 1))(expert_ids_keys, expert_ids_turns).reshape((TOKENS, TOP_K))
    route_weights = jnp.clip(jnp.exp(math.log(1.0) - 1.3862944 * jax.random.uniform(arg_keys[9], (TOKENS, TOP_K), jnp.float32) ** steps_of(arg_keys[9], (TOKENS, TOP_K), ((0, 8),), -0.2, 0.2)), 0.25, 1.0)
    return {"tokens": tokens, "norm_gain": norm_gain, "expert_gate": expert_gate, "expert_up": expert_up, "expert_down": expert_down, "shared_gate": shared_gate, "shared_up": shared_up, "shared_down": shared_down, "expert_ids": expert_ids, "route_weights": route_weights}


EPS = 1e-06

def reference(tokens, norm_gain, expert_gate, expert_up, expert_down, shared_gate, shared_up, shared_down, expert_ids, route_weights):
    gain = norm_gain.astype(jnp.float32)
    gate_ready = (expert_gate * gain[None, :, None]).astype(jnp.bfloat16)
    up_ready = (expert_up * gain[None, :, None]).astype(jnp.bfloat16)
    down_ready = expert_down.astype(jnp.bfloat16)
    shared_gate_ready = (shared_gate * gain[:, None]).astype(jnp.bfloat16)
    shared_up_ready = (shared_up * gain[:, None]).astype(jnp.bfloat16)
    shared_down_ready = shared_down.astype(jnp.bfloat16)
    wide = tokens.astype(jnp.float32)
    normed = (wide * lax.rsqrt(lax.optimization_barrier(jnp.mean(wide * wide, axis=-1, keepdims=True)) + EPS)).astype(jnp.bfloat16)
    shared_first = jnp.dot(normed, shared_gate_ready, preferred_element_type=jnp.float32)
    shared_second = jnp.dot(normed, shared_up_ready, preferred_element_type=jnp.float32)
    shared_hidden = (jax.nn.silu(shared_first) * shared_second).astype(jnp.bfloat16)
    shared_out = jnp.dot(shared_hidden, shared_down_ready, preferred_element_type=jnp.float32)
    experts = expert_gate.shape[0]
    tok_block = tokens.shape[0] // N_FS
    capacity = 2 * tok_block * TOP_K // experts
    chosen = expert_ids.reshape(N_FS, tok_block * TOP_K).astype(jnp.int32)
    onehot = (chosen[..., None] == jnp.arange(experts, dtype=jnp.int32)).astype(jnp.int32)
    ranks = (lax.optimization_barrier(jnp.sum(jnp.cumsum(onehot, axis=1) * onehot, axis=-1)) - 1).astype(jnp.int32)
    blocks = jnp.broadcast_to(jnp.arange(N_FS, dtype=jnp.int32)[:, None], chosen.shape)
    owners = (blocks * tok_block + jnp.arange(tok_block * TOP_K, dtype=jnp.int32)[None, :] // TOP_K).astype(jnp.int32)
    slot_token = jnp.zeros((experts, N_FS, capacity), jnp.int32).at[chosen, blocks, ranks].set(owners)
    slot_weight = jnp.zeros((experts, N_FS, capacity), jnp.float32).at[chosen, blocks, ranks].set(route_weights.reshape(N_FS, -1).astype(jnp.float32))

    def one_expert(total, index):
        which = slot_token[index].reshape(-1)
        rows = normed[which]
        first = jnp.dot(rows, gate_ready[index], preferred_element_type=jnp.float32)
        second = jnp.dot(rows, up_ready[index], preferred_element_type=jnp.float32)
        hidden = (jax.nn.silu(first) * second).astype(jnp.bfloat16)
        result = jnp.dot(hidden, down_ready[index], preferred_element_type=jnp.float32).astype(jnp.bfloat16)
        result = lax.optimization_barrier(result).astype(jnp.float32)
        return (total.at[which].add(result * slot_weight[index].reshape(-1)[:, None]), None)
    routed, _ = lax.scan(one_expert, jnp.zeros(tokens.shape, jnp.float32), jnp.arange(experts, dtype=jnp.int32))
    mixed = (shared_out + routed).astype(jnp.bfloat16)
    return (gate_ready, up_ready, down_ready, shared_gate_ready, shared_up_ready, shared_down_ready, mixed)
```

```python
import functools
import jax
import jax.numpy as jnp
from jax import lax
from jax.experimental import pallas as pl
from jax.experimental.pallas import tpu as pltpu
from jax.sharding import PartitionSpec as P

TOP_K = 8


EPS = 1e-06

MESH = pl.DeviceIdType.MESH
LANES = 128
VMEM_BYTES = 44 * 1024 * 1024
scope = jax.named_scope


def flip(value, mask, extent):
    result, bit = 0, 1
    while bit < extent:
        digit = (value // bit) % 2
        result = result + bit * ((1 - digit) if mask & bit else digit)
        bit *= 2
    return result


def fused_kernel(
    groups,
    ranks,
    tokens,
    gain,
    ids,
    weights,
    eg,
    eu,
    ed,
    sg,
    su,
    sd,
    rv_g,
    rv_u,
    rv_d,
    sh,
    shid,
    own_out,
    zr,
    tok_v,
    gain_v,
    ids_v,
    weights_v,
    sg_v,
    su_v,
    sd_v,
    gain_b,
    table_v,
    st_g,
    st_u,
    st_d,
    sb_g,
    sb_u,
    sb_d,
    tok,
    hid,
    xs,
    xr,
    zs,
    acc,
    load_sem,
    a2a_send,
    a2a_recv,
    tok_send,
    tok_recv,
    tok_tsend,
    tok_trecv,
    sh_send,
    sh_recv,
    hid_csend,
    hid_ysend,
    hid_fsend,
    hid_recv,
    shid_send,
    shid_recv,
    x_send,
    x_recv,
    z_send,
    z_recv,
):
    nx = 2
    me = lax.axis_index("fs")
    tp = lax.axis_index("tp")
    z, x = me // nx, me % nx
    partner = flip(tp, 1, ranks)
    across = flip(tp, 2, ranks)
    per = eg.shape[0] // groups
    experts = eg.shape[0]
    rows_w = eg.shape[1]
    rows_d = ed.shape[1]
    tok_count, features = tokens.shape
    share = tok_count // ranks
    hcols = eg.shape[2]
    dcols = ed.shape[2]
    hw = dcols // 2
    parts = ((0, hw), (hw, hw // 2), (hw + hw // 2, hw // 2))
    inn = ((z + 1) // 2) % 2
    inner, edge = inn == 1, inn == 0
    near, side, far_in, far_out = (flip(me, m, groups) for m in (2, 1, 6, 4))
    far = (inn * far_in + (1 - inn) * far_out, inn * far_out + (1 - inn) * far_in)

    pairs = (
        (gain, gain_v),
        (ids, ids_v),
        (weights, weights_v),
        (tokens, tok_v),
        (eg, st_g),
        (eu, st_u),
        (sg, sg_v),
        (su, su_v),
        (sd, sd_v),
        (ed, st_d),
    )
    loads = [pltpu.make_async_copy(a, b, load_sem.at[i]) for i, (a, b) in enumerate(pairs)]
    for load in loads:
        load.start()

    barrier = pltpu.get_barrier_semaphore()
    for o in range(1, groups):
        pl.semaphore_signal(
            barrier, inc=1, device_id={"fs": flip(me, o, groups)}, device_id_type=MESH
        )
    for o in range(1, ranks):
        pl.semaphore_signal(
            barrier, inc=1, device_id={"tp": flip(tp, o, ranks)}, device_id_type=MESH
        )

    def cast(stage, sendbuf, scaled, piece):
        @pl.loop(0, groups)
        def _(owner):
            e = owner * per + piece
            value = stage[e]
            if scaled:
                value = value * gain_b[...]
            sendbuf[e] = value.astype(jnp.bfloat16)

    mine = pl.ds(tp * share, share)
    theirs = pl.ds(across * share, share)

    def fs_copy(src, dst, send, recv, target):
        return pltpu.make_async_remote_copy(
            src_ref=src,
            dst_ref=dst,
            send_sem=send,
            recv_sem=recv,
            device_id={"fs": target},
            device_id_type=MESH,
        )

    def tp_copy(src, dst, send, recv, target):
        return pltpu.make_async_remote_copy(
            src_ref=src,
            dst_ref=dst,
            send_sem=send,
            recv_sem=recv,
            device_id={"tp": target},
            device_id_type=MESH,
        )

    ways = (near, side, far_in)

    def tok_copy(way, block):
        ref = tok.at[block, mine]
        return fs_copy(ref, ref, tok_send.at[way, block], tok_recv.at[block], ways[way])

    def sh_copy(way, block, part):
        ref = sh.at[block, part]
        return fs_copy(
            ref, ref, sh_send.at[way, block, part], sh_recv.at[block, part], ways[way]
        )

    def if_inner(act):
        pl.when(inner)(act)

    def tok_share(kind, block):
        rows = theirs if kind == 2 else mine
        return tp_copy(
            tok.at[block, rows],
            tok.at[block, rows],
            tok_tsend.at[kind, block],
            tok_trecv.at[kind, block],
            across if kind == 1 else partner,
        )

    def tok_arrive(block):
        tok_copy(0, block).wait_recv()
        tok_share(0, block).start()
        tok_share(1, block).start()

    def tok_moves(stage, act):
        if stage == 0:
            if_inner(lambda: act(tok_copy(2, me)))
            act(tok_copy(0, me))
            act(tok_copy(1, me))
        elif stage == 1:
            if_inner(lambda: act(tok_copy(2, near)))
            act(tok_copy(1, near))
        else:
            if_inner(lambda: act(tok_copy(0, far[stage - 2])))
            act(tok_copy(1, far[stage - 2]))

    def start(c):
        c.start()

    def wait_send(c):
        c.wait_send()

    order = (6, 7, 4, 5, 2, 3, 1)

    def a2a_ends(index, piece, owner_at, row_at):
        if index < 2:
            sendbuf, recvbuf = ((sb_g, rv_g), (sb_u, rv_u))[index]
            return (
                sendbuf.at[owner_at * per + piece],
                recvbuf.at[piece, pl.ds(row_at * rows_w, rows_w), :],
            )
        columns = pl.ds(*parts[piece])
        return (
            sb_d.at[pl.ds(owner_at * per, per), :, columns],
            rv_d.at[:, pl.ds(row_at * rows_d, rows_d), columns],
        )

    def a2a_copy(index, piece, o):
        target = flip(me, o, groups)
        src, dst = a2a_ends(index, piece, target, me)
        return fs_copy(
            src, dst, a2a_send.at[index, piece, o], a2a_recv.at[index, piece, o], target
        )

    def a2a_start(index, piece):
        for o in order:
            a2a_copy(index, piece, o).start()

    def a2a_own(index, piece):
        src, dst = a2a_ends(index, piece, me, me)
        dst[...] = src[...]

    def a2a_arrive(index, piece):
        for o in order:
            a2a_copy(index, piece, o).wait_recv()

    def far_start(index, piece):
        for o in order[:4]:
            a2a_copy(index, piece, o).start()

    def close_start(index, piece):
        for o in order[4:]:
            a2a_copy(index, piece, o).start()

    with scope("gain"):
        loads[0].wait()
        at_row = lax.broadcasted_iota(jnp.int32, (rows_w, rows_w), 0)
        at_column = lax.broadcasted_iota(jnp.int32, (rows_w, rows_w), 1)
        column = jnp.sum(
            jnp.where(at_row == at_column, gain_v[...], 0.0), axis=1, keepdims=True
        )
        gain_b[...] = jnp.broadcast_to(column, (rows_w, hcols))

    with scope("table"):
        loads[1].wait()
        loads[2].wait()
        row = lax.broadcasted_iota(jnp.int32, (experts, tok_count), 0)
        table = jnp.zeros((experts, tok_count), jnp.float32)
        for k in range(ids.shape[0]):
            table = table + jnp.where(row == ids_v[k : k + 1, :], weights_v[k : k + 1, :], 0.0)
        high = table.astype(jnp.bfloat16).astype(jnp.float32)
        middle = (table - high).astype(jnp.bfloat16).astype(jnp.float32)
        table_v[...] = jnp.zeros(table_v.shape, jnp.float32)
        for i, value in enumerate((high, middle, table - high - middle)):
            table_v[i * experts : (i + 1) * experts, 0:tok_count] = value
        tok[me, :, features : features + LANES] = table_v[...].T[0:tok_count].astype(jnp.bfloat16)

    def norm(first, count):
        @pl.loop(0, count // 16)
        def _(i):
            rows = pl.ds(first + i * 16, 16)
            wide = tok_v[rows, :].astype(jnp.float32)
            mean = jnp.mean(wide * wide, axis=-1, keepdims=True)
            tok[me, rows, 0:features] = (wide * lax.rsqrt(mean + EPS)).astype(jnp.bfloat16)

    with scope("norm"):
        loads[3].wait()
        norm(tp * share, share)

    with scope("barrier"):
        pl.semaphore_wait(barrier, groups + ranks - 2)

    with scope("launch"):
        tok_moves(0, start)
        loads[4].wait()
        cast(st_g, sb_g, True, 0)

        @pl.when(edge)
        def _():
            far_start(0, 0)

        close_start(0, 0)
        for o in range(1, ranks):
            norm(flip(tp, o, ranks) * share, share)
        loads[5].wait()
        cast(st_u, sb_u, True, 0)
    with scope("near_tokens"):
        tok_arrive(near)
        tok_moves(1, start)

        @pl.when(inner)
        def _():
            far_start(0, 0)

        far_start(1, 0)
        close_start(1, 0)
    with scope("casts"):
        for i in range(6, 10):
            loads[i].wait()
        sh[me, 0] = (sg_v[...] * gain_b[...]).astype(jnp.bfloat16)
        sh[me, 1] = (su_v[...] * gain_b[...]).astype(jnp.bfloat16)
        sh[me, 2, 0:rows_d] = sd_v[:, 0:hw].astype(jnp.bfloat16)
        sh[me, 2, rows_d : 2 * rows_d] = sd_v[:, hw:dcols].astype(jnp.bfloat16)
        for piece in range(1, per):
            cast(st_g, sb_g, True, piece)
            cast(st_u, sb_u, True, piece)
        for piece in range(per):
            cast(st_d, sb_d, False, piece)
        for index in range(2):
            for piece in range(per):
                a2a_own(index, piece)
        for piece in range(len(parts)):
            a2a_own(2, piece)
    with scope("far_tokens0"):
        tok_arrive(far[0])
        tok_moves(2, start)
    with scope("far_tokens1"):
        tok_arrive(far[1])
        tok_moves(3, start)
        for part in range(3):
            sh_copy(0, me, part).start()
            sh_copy(1, me, part).start()
        for part in range(2):
            if_inner(lambda: sh_copy(2, me, part).start())
    with scope("side_tokens"):
        for m in (1, 3, 5, 7):
            tok_arrive(flip(me, m, groups))
    with scope("near_shared"):
        for part in range(3):
            sh_copy(0, near, part).wait_recv()
            if part < 2:
                if_inner(lambda: sh_copy(2, near, part).start())
            sh_copy(1, near, part).start()
    with scope("arrive_g0"):
        a2a_arrive(0, 0)
        a2a_start(0, 1)
    with scope("shares"):
        for o in range(1, groups):
            tok_share(1, flip(me, o, groups)).wait_recv()
            tok_share(2, flip(me, o, groups)).start()
        for o in range(1, groups):
            tok_share(0, flip(me, o, groups)).wait_recv()
            tok_share(2, flip(me, o, groups)).wait_recv()

    def far_shared(k, part):
        sh_copy(0, far[k], part).wait_recv()
        if_inner(lambda: sh_copy(0, far[k], part).start())
        sh_copy(1, far[k], part).start()

    def far_shared_start(part):
        for block in (me, near):
            if_inner(lambda: sh_copy(2, block, part).start())

    def shared_sum(part, blocks):
        total = jnp.zeros((tok_count, hcols), jnp.float32)
        for block in blocks:
            columns = pl.ds(pl.multiple_of(block * rows_w, rows_w), rows_w)
            total = total + jnp.dot(
                tok[me, :, columns], sh[block, part], preferred_element_type=jnp.float32
            )
        return total

    def shid_copy(o):
        return tp_copy(
            shid.at[tp], shid.at[tp], shid_send.at[o], shid_recv.at[o], flip(tp, o, ranks)
        )

    def hid_core(e, block):
        return tp_copy(
            hid.at[tp, block, e],
            hid.at[tp, block, e],
            hid_csend.at[e, block],
            hid_recv.at[0, e, block],
            partner,
        )

    def hid_across(e, block):
        return tp_copy(
            hid.at[tp, block, e],
            hid.at[tp, block, e],
            hid_ysend.at[e, block],
            hid_recv.at[1, e, block],
            across,
        )

    def hid_forward(e, block):
        return tp_copy(
            hid.at[across, block, e],
            hid.at[across, block, e],
            hid_fsend.at[e, block],
            hid_recv.at[2, e, block],
            partner,
        )

    def turn(o):
        return (me + o) % groups

    for e in range(per):
        with scope(f"arrive_u{e}"):
            if e == 1:
                a2a_arrive(0, 1)
                a2a_start(2, 0)
            a2a_arrive(1, e)
            if e == 0:
                a2a_start(1, 1)
            else:
                a2a_start(2, 1)
                a2a_start(2, 2)
                far_shared_start(2)
        with scope(f"hidden{e}"):

            @pl.loop(0, groups)
            def _(o):
                block = turn(o + 1)
                rows = tok[block, :, 0:features]
                first = jnp.dot(rows, rv_g[e], preferred_element_type=jnp.float32)
                second = jnp.dot(rows, rv_u[e], preferred_element_type=jnp.float32)
                hid[tp, block, e] = (jax.nn.silu(first) * second).astype(jnp.bfloat16)

                @pl.when(o >= 1)
                def _():
                    before = turn(o)
                    hid_across(e, before).start()
                    hid_core(e, before).start()

            hid_across(e, me).start()
            hid_core(e, me).start()
        if e == 0:
            with scope("far_shared_gu"):
                for k in range(2):
                    for part in range(2):
                        far_shared(k, part)
        with scope(f"forward{e}"):

            @pl.loop(0, groups)
            def _(o):
                block = turn(o + 1)
                hid_across(e, block).wait_recv()
                hid_forward(e, block).start()

        if e == 0:
            with scope("side_shared_gu"):
                for part in range(2):
                    for m in (1, 3, 5, 7):
                        sh_copy(1, flip(me, m, groups), part).wait_recv()
            with scope("shared_hidden"):
                first, second = (shared_sum(part, range(groups)) for part in range(2))
                shid[tp] = (jax.nn.silu(first) * second).astype(jnp.bfloat16)
                for stage in range(4):
                    tok_moves(stage, wait_send)
                for o in range(1, groups):
                    for kind in range(3):
                        tok_share(kind, flip(me, o, groups)).wait_send()
                for o in range(1, ranks):
                    shid_copy(o).start()

    with scope("hid_wait"):

        @pl.loop(1, groups + 1)
        def _(o):
            block = turn(o)
            for e in range(per):
                hid_core(e, block).wait_recv()
                hid_forward(e, block).wait_recv()

        @pl.loop(0, groups)
        def _(o):
            for e in range(per):
                hid_core(e, o).wait_send()
                hid_across(e, o).wait_send()
                hid_forward(e, o).wait_send()

    lanes = lax.broadcasted_iota(jnp.int32, (tok_count, LANES), 1)

    def block_out(block, part):
        offset, wide = parts[part]
        table = tok[block, :, features : features + LANES].astype(jnp.float32)
        total = jnp.zeros((tok_count, wide), jnp.float32)
        for e in range(per):
            expert = me * per + e
            weight = jnp.sum(
                jnp.where(
                    (lanes == expert) | (lanes == expert + experts) | (lanes == expert + 2 * experts),
                    table,
                    0.0,
                ),
                axis=1,
                keepdims=True,
            )
            out = jnp.zeros((tok_count, wide), jnp.float32)
            for r in range(ranks):
                out = out + jnp.dot(
                    hid[r, block, e],
                    rv_d[e, r * hcols : (r + 1) * hcols, offset : offset + wide],
                    preferred_element_type=jnp.float32,
                )
            total = total + weight * out
        return total

    def dest(k):
        step = (k + 2 * inn) % 4
        half = z // 2
        away = 1 - step // 2
        chosen = half * (1 - away) + (1 - half) * away
        is_inner = (step % 2) * (1 - away) * inn + (1 - step % 2) * (1 - away) * (1 - inn) + (1 - step % 2) * away
        return chosen * (3 - is_inner) + (1 - chosen) * is_inner

    def x_copy(part, k):
        columns = pl.ds(*parts[part])
        return fs_copy(
            xs.at[k, :, columns], xr.at[k, :, columns], x_send.at[part, k], x_recv.at[part, k], side
        )

    def z_copy(part, k, slot, target):
        columns = pl.ds(*parts[part])
        return fs_copy(
            zs.at[k, :, columns],
            zr.at[slot, :, columns],
            z_send.at[part, k],
            z_recv.at[part, slot],
            target,
        )

    def x_stage(part):
        columns = pl.ds(*parts[part])

        @pl.loop(0, 4)
        def _(k):
            xs[k, :, columns] = block_out(dest(k) * nx + 1 - x, part).astype(jnp.bfloat16)

            @pl.when(k >= 1)
            def _():
                x_copy(part, k - 1).start()

    def z_stage(part):
        columns = pl.ds(*parts[part])

        @pl.loop(0, 4)
        def _(k):
            total = block_out(dest(k) * nx + x, part)

            @pl.when(k == 0)
            def _():
                x_copy(part, 3).start()

            x_copy(part, k).wait_recv()
            total = total + xr[k, :, columns].astype(jnp.float32)
            acc[k, :, columns] = total
            zs[k, :, columns] = total.astype(jnp.bfloat16)

            @pl.when((k >= 1) & edge)
            def _():
                z_copy(part, k - 1, k + 1, near).start()

            @pl.when((k == 1) & inner)
            def _():
                z_copy(part, 0, 4, near).start()

    def z_join(part):
        columns = pl.ds(*parts[part])

        @pl.when(inner)
        def _():
            for k in (2, 3):
                z_copy(part, k, k, near).wait_recv()
                zs[k, :, columns] = (
                    acc[k, :, columns] + zr[k, :, columns].astype(jnp.float32)
                ).astype(jnp.bfloat16)
            own_out[:, columns] = acc[1, :, columns]
            z_copy(part, 2, 5, far_in).start()
            z_copy(part, 3, 5, far_out).start()

        @pl.when(edge)
        def _():
            own_out[:, columns] = acc[3, :, columns]

    for part in range(len(parts)):
        with scope(f"arrive_d{part}"):
            a2a_arrive(2, part)
        with scope(f"x_stage{part}"):
            x_stage(part)
        with scope(f"z_stage{part}"):
            z_stage(part)
        if part == len(parts) - 1:
            with scope("far_shared_d0"):
                far_shared(0, 2)
        with scope(f"z_join{part}"):
            z_join(part)
    with scope("far_shared_d1"):
        far_shared(1, 2)
    with scope("side_shared_d"):
        for m in (1, 3, 5, 7):
            sh_copy(1, flip(me, m, groups), 2).wait_recv()
    with scope("drain"):
        for index in range(3):
            for piece in range(per if index < 2 else len(parts)):
                for o in order:
                    a2a_copy(index, piece, o).wait_send()
        for part in range(3):
            for way in range(2):
                sh_copy(way, me, part).wait_send()
            sh_copy(1, near, part).wait_send()
            for k in range(2):
                if_inner(lambda: sh_copy(0, far[k], part).wait_send())
                sh_copy(1, far[k], part).wait_send()
            for block in (me, near):
                if_inner(lambda: sh_copy(2, block, part).wait_send())
        for part in range(len(parts)):
            for k in range(4):
                x_copy(part, k).wait_send()
            for k in range(3):

                @pl.when(edge)
                def _():
                    z_copy(part, k, k + 2, near).wait_send()

            @pl.when(inner)
            def _():
                for k in (0, 2, 3):
                    z_copy(part, k, 4, near).wait_send()

    with scope("last"):
        for part in range(len(parts)):
            for slot in (4, 5):
                z_copy(part, 0, slot, near).wait_recv()
        for o in range(1, ranks):
            shid_copy(o).wait_recv()
            shid_copy(o).wait_send()


def finish_kernel(
    rv_g, rv_u, rv_d, sh, shid, own_out, zr, gate, up, down, sgate, sup, sdown, mixed, mixed_v, sems
):
    rows_d, hw = sdown.shape[1], sdown.shape[2] // 2
    groups, hcols = sh.shape[0], shid.shape[2]
    moves = [
        (rv_g, gate),
        (rv_u, up),
        (rv_d, down),
        (sh.at[:, 0], sgate),
        (sh.at[:, 1], sup),
        (sh.at[:, 2, pl.ds(0, rows_d)], sdown.at[:, :, pl.ds(0, hw)]),
        (sh.at[:, 2, pl.ds(rows_d, rows_d)], sdown.at[:, :, pl.ds(hw, hw)]),
    ]
    copies = [pltpu.make_async_copy(a, b, sems.at[i]) for i, (a, b) in enumerate(moves)]
    for copy in copies:
        copy.start()
    for part in range(2):
        columns = slice(part * hw, (part + 1) * hw)
        total = own_out[:, columns]
        for slot in (4, 5):
            total = total + zr[slot, :, columns].astype(jnp.float32)
        for block in range(groups):
            at = block * rows_d
            total = total + jnp.dot(
                shid[at // hcols, :, at % hcols : at % hcols + rows_d],
                sh[block, 2, part * rows_d : (part + 1) * rows_d],
                preferred_element_type=jnp.float32,
            )
        mixed_v[:, columns] = total.astype(jnp.bfloat16)
    last = pltpu.make_async_copy(mixed_v, mixed, sems.at[len(moves)])
    last.start()
    for copy in copies:
        copy.wait()
    last.wait()


def dense_body(
    tokens,
    norm_gain,
    expert_gate,
    expert_up,
    expert_down,
    shared_gate,
    shared_up,
    shared_down,
    expert_ids,
    route_weights,
):
    groups, ranks = lax.axis_size("fs"), lax.axis_size("tp")
    experts, rows_w, hcols = expert_gate.shape
    rows_d, dcols = expert_down.shape[1:]
    per = experts // groups
    tok_count, features = tokens.shape
    total = features + LANES
    bf, f32 = jnp.bfloat16, jnp.float32
    dma = pltpu.SemaphoreType.DMA
    any_space = pl.BlockSpec(memory_space=pl.ANY)
    vmem = pl.BlockSpec(memory_space=pltpu.VMEM)
    hidden = hcols * ranks
    wide_rows = -(-tok_count // LANES) * LANES
    made = pl.pallas_call(
        functools.partial(fused_kernel, groups, ranks),
        out_shape=(
            pltpu.VMEM((per, features, hcols), bf),
            pltpu.VMEM((per, features, hcols), bf),
            pltpu.VMEM((per, hidden, dcols), bf),
            pltpu.VMEM((groups, 3, rows_w, hcols), bf),
            pltpu.VMEM((ranks, tok_count, hcols), bf),
            pltpu.VMEM((tok_count, dcols), f32),
            pltpu.VMEM((6, tok_count, dcols), bf),
        ),
        in_specs=[any_space] * 10,
        out_specs=(vmem,) * 7,
        scratch_shapes=[
            pltpu.VMEM((tok_count, features), bf),
            pltpu.VMEM((1, rows_w), f32),
            pltpu.VMEM((TOP_K, tok_count), jnp.int32),
            pltpu.VMEM((TOP_K, tok_count), f32),
            pltpu.VMEM((rows_w, hcols), f32),
            pltpu.VMEM((rows_w, hcols), f32),
            pltpu.VMEM((rows_d, dcols), f32),
            pltpu.VMEM((rows_w, hcols), f32),
            pltpu.VMEM((LANES, wide_rows), f32),
            pltpu.VMEM((experts, rows_w, hcols), f32),
            pltpu.VMEM((experts, rows_w, hcols), f32),
            pltpu.VMEM((experts, rows_d, dcols), f32),
            pltpu.VMEM((experts, rows_w, hcols), bf),
            pltpu.VMEM((experts, rows_w, hcols), bf),
            pltpu.VMEM((experts, rows_d, dcols), bf),
            pltpu.VMEM((groups, tok_count, total), bf),
            pltpu.VMEM((ranks, groups, per, tok_count, hcols), bf),
            pltpu.VMEM((4, tok_count, dcols), bf),
            pltpu.VMEM((4, tok_count, dcols), bf),
            pltpu.VMEM((4, tok_count, dcols), bf),
            pltpu.VMEM((4, tok_count, dcols), f32),
            dma((10,)),
            dma((3, max(per, 3), groups)),
            dma((3, max(per, 3), groups)),
            dma((3, groups)),
            dma((groups,)),
            dma((3, groups)),
            dma((3, groups)),
            dma((3, groups, 3)),
            dma((groups, 3)),
            dma((per, groups)),
            dma((per, groups)),
            dma((per, groups)),
            dma((3, per, groups)),
            dma((ranks,)),
            dma((ranks,)),
            dma((3, 4)),
            dma((3, 4)),
            dma((3, 4)),
            dma((3, 6)),
        ],
        compiler_params=pltpu.CompilerParams(
            collective_id=0, has_side_effects=True, vmem_limit_bytes=VMEM_BYTES
        ),
    )(
        tokens,
        norm_gain[None, :],
        expert_ids.T,
        route_weights.T,
        expert_gate,
        expert_up,
        expert_down,
        shared_gate,
        shared_up,
        shared_down,
    )
    gate, up, down, sgate, sup, sdown, mixed = pl.pallas_call(
        finish_kernel,
        out_shape=tuple(
            jax.ShapeDtypeStruct(shape, bf)
            for shape in (
                (per, features, hcols),
                (per, features, hcols),
                (per, hidden, dcols),
                (groups, rows_w, hcols),
                (groups, rows_w, hcols),
                (groups, rows_d, dcols),
                (tok_count, dcols),
            )
        ),
        in_specs=[vmem] * 7,
        out_specs=(any_space,) * 7,
        scratch_shapes=[pltpu.VMEM((tok_count, dcols), bf), dma((8,))],
        compiler_params=pltpu.CompilerParams(vmem_limit_bytes=VMEM_BYTES // 4),
    )(*made)
    return (
        gate,
        up,
        down,
        sgate.reshape(features, hcols),
        sup.reshape(features, hcols),
        sdown.reshape(hidden, dcols),
        mixed,
    )


def expert_hidden(rows, gate_new, up_new):
    first = jnp.einsum("secn,enf->secf", rows, gate_new, preferred_element_type=jnp.float32)
    second = jnp.einsum("secn,enf->secf", rows, up_new, preferred_element_type=jnp.float32)
    return (jax.nn.silu(first) * second).astype(jnp.bfloat16)


def body(
    tokens,
    norm_gain,
    expert_gate,
    expert_up,
    expert_down,
    shared_gate,
    shared_up,
    shared_down,
    expert_ids,
    route_weights,
):
    groups = lax.axis_size("fs")
    experts = expert_gate.shape[0]
    per_group = experts // groups
    tok_count = tokens.shape[0]
    capacity = 2 * tok_count * TOP_K // experts
    ranks = lax.axis_size("tp")
    square = expert_down.shape[1] * expert_down.shape[2] == shared_gate.size
    if capacity >= tok_count and per_group >= 2 and groups == 8 and ranks == 4 and square:
        return dense_body(
            tokens,
            norm_gain,
            expert_gate,
            expert_up,
            expert_down,
            shared_gate,
            shared_up,
            shared_down,
            expert_ids,
            route_weights,
        )
    gate_local = (expert_gate * norm_gain[None, :, None]).astype(jnp.bfloat16)
    up_local = (expert_up * norm_gain[None, :, None]).astype(jnp.bfloat16)
    down_local = expert_down.astype(jnp.bfloat16)
    gate_local = gate_local.reshape((groups, per_group) + gate_local.shape[1:])
    up_local = up_local.reshape((groups, per_group) + up_local.shape[1:])
    down_local = down_local.reshape((groups, per_group) + down_local.shape[1:])
    shared_first_local = (shared_gate * norm_gain[:, None]).astype(jnp.bfloat16)
    shared_second_local = (shared_up * norm_gain[:, None]).astype(jnp.bfloat16)
    shared_third_local = shared_down.astype(jnp.bfloat16)
    gate_moved, up_moved, down_moved = (
        lax.all_to_all(gate_local, "fs", split_axis=0, concat_axis=2, tiled=True),
        lax.all_to_all(up_local, "fs", split_axis=0, concat_axis=2, tiled=True),
        lax.all_to_all(down_local, "fs", split_axis=0, concat_axis=2, tiled=True),
    )
    down_ready = down_moved[0]
    gate_ready = gate_moved[0]
    up_ready = up_moved[0]
    shared_gate_ready, shared_up_ready, shared_down_ready = (
        lax.all_gather(shared_first_local, "fs", axis=0, tiled=True),
        lax.all_gather(shared_second_local, "fs", axis=0, tiled=True),
        lax.all_gather(shared_third_local, "fs", axis=0, tiled=True),
    )
    wide = tokens.astype(jnp.float32)
    normed = (wide * lax.rsqrt(jnp.mean(wide * wide, axis=-1, keepdims=True) + EPS)).astype(
        jnp.bfloat16
    )
    chosen = expert_ids.reshape(-1)
    onehot = (chosen[:, None] == jnp.arange(experts, dtype=jnp.int32)[None, :]).astype(jnp.int32)
    ranks = jnp.sum(jnp.cumsum(onehot, axis=0) * onehot, axis=1) - 1
    owners = jnp.arange(tok_count * TOP_K, dtype=jnp.int32) // TOP_K
    slot_token = jnp.zeros((experts, capacity), jnp.int32).at[chosen, ranks].set(owners)
    outgoing = normed[slot_token.reshape(-1)].reshape(groups, per_group, capacity, normed.shape[1])
    share = capacity // lax.axis_size("tp")
    mine = lax.dynamic_slice_in_dim(outgoing, lax.axis_index("tp") * share, share, 2)
    arrived = lax.all_to_all(mine, "fs", split_axis=0, concat_axis=0, tiled=True)
    hidden = expert_hidden(lax.all_gather(arrived, "tp", axis=2, tiled=True), gate_ready, up_ready)
    shared_first = jnp.dot(normed, shared_gate_ready, preferred_element_type=jnp.float32)
    shared_second = jnp.dot(normed, shared_up_ready, preferred_element_type=jnp.float32)
    shared_hidden = (jax.nn.silu(shared_first) * shared_second).astype(jnp.bfloat16)[None, None]
    columns = down_ready.shape[2]
    routed_piece = lax.all_gather(hidden, "tp", axis=3, tiled=True)
    shared_piece = lax.all_gather(shared_hidden, "tp", axis=3, tiled=True)
    routed_total = jnp.einsum(
        "secf,efd->secd", routed_piece, down_ready, preferred_element_type=jnp.float32
    )
    shared_total = jnp.einsum(
        "abtf,fd->abtd", shared_piece, shared_down_ready, preferred_element_type=jnp.float32
    )
    returned = lax.all_to_all(
        routed_total.astype(jnp.bfloat16), "fs", split_axis=0, concat_axis=0, tiled=True
    )
    returned = returned.reshape(experts * capacity, columns)
    picked = (
        returned[chosen * capacity + ranks].astype(jnp.float32).reshape(tok_count, TOP_K, columns)
    )
    routed = jnp.sum(picked * route_weights[:, :, None], axis=1)
    mixed = (shared_total[0, 0] + routed).astype(jnp.bfloat16)
    return (
        gate_ready,
        up_ready,
        down_ready,
        shared_gate_ready,
        shared_up_ready,
        shared_down_ready,
        mixed,
    )


def solution(mesh):
    in_specs = (
        P("fs", None),
        P("fs"),
        P(None, "fs", "tp"),
        P(None, "fs", "tp"),
        P(None, "fs", "tp"),
        P("fs", "tp"),
        P("fs", "tp"),
        P("fs", "tp"),
        P("fs", None),
        P("fs", None),
    )
    out_specs = (
        P("fs", None, "tp"),
        P("fs", None, "tp"),
        P("fs", None, "tp"),
        P(None, "tp"),
        P(None, "tp"),
        P(None, "tp"),
        P("fs", "tp"),
    )
    return jax.shard_map(body, mesh=mesh, in_specs=in_specs, out_specs=out_specs, check_vma=False)
```

```python
import functools
import jax
import jax.numpy as jnp
from jax import lax
from jax.experimental import pallas as pl
from jax.experimental.pallas import tpu as pltpu
from jax.sharding import PartitionSpec as P

TOP_K = 8


EPS = 1e-06

MESH = pl.DeviceIdType.MESH
LANES = 128
VMEM_BYTES = 44 * 1024 * 1024
scope = jax.named_scope


def flip(value, mask, extent):
    result, bit = 0, 1
    while bit < extent:
        digit = (value // bit) % 2
        result = result + bit * ((1 - digit) if mask & bit else digit)
        bit *= 2
    return result


def fused_kernel(
    groups,
    ranks,
    tokens,
    gain,
    ids,
    weights,
    eg,
    eu,
    ed,
    sg,
    su,
    sd,
    rv_g,
    rv_u,
    rv_d,
    sh,
    shid,
    own_out,
    zr,
    tok_v,
    gain_v,
    ids_v,
    weights_v,
    sg_v,
    su_v,
    sd_v,
    gain_b,
    table_v,
    st_g,
    st_u,
    st_d,
    sb_g,
    sb_u,
    sb_d,
    tok,
    hid,
    xs,
    xr,
    zs,
    acc,
    load_sem,
    a2a_send,
    a2a_recv,
    tok_send,
    tok_recv,
    tok_tsend,
    tok_trecv,
    tok_yrecv,
    sh_send,
    sh_recv,
    hid_send,
    hid_recv,
    hid_yrecv,
    shid_send,
    shid_recv,
    x_send,
    x_recv,
    z_send,
    z_recv,
):
    nx = 2
    me = lax.axis_index("fs")
    tp = lax.axis_index("tp")
    z, x = me // nx, me % nx
    partner = flip(tp, 1, ranks)
    across = flip(tp, 2, ranks)
    per = eg.shape[0] // groups
    experts = eg.shape[0]
    rows_w = eg.shape[1]
    rows_d = ed.shape[1]
    tok_count, features = tokens.shape
    share = tok_count // ranks
    hcols = eg.shape[2]
    dcols = ed.shape[2]
    hw = dcols // 2
    parts = ((0, hw), (hw, hw // 2), (hw + hw // 2, hw // 2))
    inn = ((z + 1) // 2) % 2
    inner, edge = inn == 1, inn == 0
    near, side, far_in, far_out = (flip(me, m, groups) for m in (2, 1, 6, 4))
    far = (inn * far_in + (1 - inn) * far_out, inn * far_out + (1 - inn) * far_in)

    pairs = (
        (gain, gain_v),
        (ids, ids_v),
        (weights, weights_v),
        (tokens, tok_v),
        (eg, st_g),
        (eu, st_u),
        (sg, sg_v),
        (su, su_v),
        (sd, sd_v),
        (ed, st_d),
    )
    loads = [pltpu.make_async_copy(a, b, load_sem.at[i]) for i, (a, b) in enumerate(pairs)]
    for load in loads:
        load.start()

    barrier = pltpu.get_barrier_semaphore()
    for o in range(1, groups):
        pl.semaphore_signal(
            barrier, inc=1, device_id={"fs": flip(me, o, groups)}, device_id_type=MESH
        )
    for o in range(1, ranks):
        pl.semaphore_signal(
            barrier, inc=1, device_id={"tp": flip(tp, o, ranks)}, device_id_type=MESH
        )

    def cast(stage, sendbuf, scaled, piece):
        @pl.loop(0, groups)
        def _(owner):
            e = owner * per + piece
            value = stage[e]
            if scaled:
                value = value * gain_b[...]
            sendbuf[e] = value.astype(jnp.bfloat16)

    mine = pl.ds(tp * share, share)
    theirs = pl.ds(across * share, share)

    def fs_copy(src, dst, send, recv, target):
        return pltpu.make_async_remote_copy(
            src_ref=src,
            dst_ref=dst,
            send_sem=send,
            recv_sem=recv,
            device_id={"fs": target},
            device_id_type=MESH,
        )

    def tp_copy(src, dst, send, recv, target):
        return pltpu.make_async_remote_copy(
            src_ref=src,
            dst_ref=dst,
            send_sem=send,
            recv_sem=recv,
            device_id={"tp": target},
            device_id_type=MESH,
        )

    ways = (near, side, far_in)

    def tok_copy(way, block):
        ref = tok.at[block, mine]
        return fs_copy(ref, ref, tok_send.at[way], tok_recv.at[block], ways[way])

    def sh_copy(way, block, part):
        ref = sh.at[block, part]
        return fs_copy(
            ref, ref, sh_send.at[way], sh_recv.at[block, part], ways[way]
        )

    def if_inner(act):
        pl.when(inner)(act)

    def tok_share(kind, block):
        rows = theirs if kind == 2 else mine
        return tp_copy(
            tok.at[block, rows],
            tok.at[block, rows],
            tok_tsend.at[kind],
            tok_yrecv.at[block] if kind == 1 else tok_trecv.at[kind // 2],
            across if kind == 1 else partner,
        )

    def tok_arrive(block):
        tok_copy(0, block).wait_recv()
        tok_share(0, block).start()
        tok_share(1, block).start()

    def tok_moves(stage, act):
        if stage == 0:
            if_inner(lambda: act(tok_copy(2, me)))
            act(tok_copy(0, me))
            act(tok_copy(1, me))
        elif stage == 1:
            if_inner(lambda: act(tok_copy(2, near)))
            act(tok_copy(1, near))
        else:
            if_inner(lambda: act(tok_copy(0, far[stage - 2])))
            act(tok_copy(1, far[stage - 2]))

    def start(c):
        c.start()

    def wait_send(c):
        c.wait_send()

    order = (6, 7, 4, 5, 2, 3, 1)

    def a2a_ends(index, piece, owner_at, row_at):
        if index < 2:
            sendbuf, recvbuf = ((sb_g, rv_g), (sb_u, rv_u))[index]
            return (
                sendbuf.at[owner_at * per + piece],
                recvbuf.at[piece, pl.ds(row_at * rows_w, rows_w), :],
            )
        columns = pl.ds(*parts[piece])
        return (
            sb_d.at[pl.ds(owner_at * per, per), :, columns],
            rv_d.at[:, pl.ds(row_at * rows_d, rows_d), columns],
        )

    def a2a_copy(index, piece, o):
        target = flip(me, o, groups)
        src, dst = a2a_ends(index, piece, target, me)
        return fs_copy(
            src, dst, a2a_send.at[index], a2a_recv.at[index, piece], target
        )

    def a2a_start(index, piece):
        far_start(index, piece)
        close_start(index, piece)

    def a2a_own(index, piece):
        src, dst = a2a_ends(index, piece, me, me)
        dst[...] = src[...]

    def settle(ref, sem):
        pltpu.make_async_copy(ref, ref, sem).wait()

    def a2a_arrive(index, piece):
        others = groups - 1
        if index < 2:
            ref = (rv_g, rv_u)[index].at[piece, pl.ds(0, others * rows_w)]
        else:
            ref = rv_d.at[:, pl.ds(0, others * rows_d), pl.ds(*parts[piece])]
        settle(ref, a2a_recv.at[index, piece])

    def if_edge(act):
        pl.when(edge)(act)

    def starts(index, piece, targets):
        for o in targets:
            a2a_copy(index, piece, o).start()

    def far_start(index, piece):
        if_inner(lambda: starts(index, piece, (4, 5, 6, 7)))
        if_edge(lambda: starts(index, piece, (6, 7, 4, 5)))

    def close_start(index, piece):
        starts(index, piece, (2, 3, 1))

    with scope("gain"):
        loads[0].wait()
        at_row = lax.broadcasted_iota(jnp.int32, (rows_w, rows_w), 0)
        at_column = lax.broadcasted_iota(jnp.int32, (rows_w, rows_w), 1)
        column = jnp.sum(
            jnp.where(at_row == at_column, gain_v[...], 0.0), axis=1, keepdims=True
        )
        gain_b[...] = jnp.broadcast_to(column, (rows_w, hcols))

    with scope("table"):
        loads[1].wait()
        loads[2].wait()
        row = lax.broadcasted_iota(jnp.int32, (experts, tok_count), 0)
        table = jnp.zeros((experts, tok_count), jnp.float32)
        for k in range(ids.shape[0]):
            table = table + jnp.where(row == ids_v[k : k + 1, :], weights_v[k : k + 1, :], 0.0)
        high = table.astype(jnp.bfloat16).astype(jnp.float32)
        middle = (table - high).astype(jnp.bfloat16).astype(jnp.float32)
        table_v[...] = jnp.zeros(table_v.shape, jnp.float32)
        for i, value in enumerate((high, middle, table - high - middle)):
            table_v[i * experts : (i + 1) * experts, 0:tok_count] = value
        tok[me, :, features : features + LANES] = table_v[...].T[0:tok_count].astype(jnp.bfloat16)

    def norm(first, count):
        @pl.loop(0, count // 16)
        def _(i):
            rows = pl.ds(first + i * 16, 16)
            wide = tok_v[rows, :].astype(jnp.float32)
            mean = jnp.mean(wide * wide, axis=-1, keepdims=True)
            tok[me, rows, 0:features] = (wide * lax.rsqrt(mean + EPS)).astype(jnp.bfloat16)

    with scope("norm"):
        loads[3].wait()
        norm(tp * share, share)

    with scope("barrier"):
        pl.semaphore_wait(barrier, groups + ranks - 2)

    with scope("launch"):
        tok_moves(0, start)
        loads[4].wait()
        cast(st_g, sb_g, True, 0)

        if_edge(lambda: starts(0, 0, (6, 7, 4, 5)))
        close_start(0, 0)
        for o in range(1, ranks):
            norm(flip(tp, o, ranks) * share, share)
        loads[5].wait()
        cast(st_u, sb_u, True, 0)
    with scope("near_tokens"):
        tok_arrive(near)
        tok_moves(1, start)

        if_inner(lambda: starts(0, 0, (4, 5, 6, 7)))
        far_start(1, 0)
        close_start(1, 0)
    with scope("casts"):
        for i in range(6, 10):
            loads[i].wait()
        sh[me, 0] = (sg_v[...] * gain_b[...]).astype(jnp.bfloat16)
        sh[me, 1] = (su_v[...] * gain_b[...]).astype(jnp.bfloat16)
        sh[me, 2, 0:rows_d] = sd_v[:, 0:hw].astype(jnp.bfloat16)
        sh[me, 2, rows_d : 2 * rows_d] = sd_v[:, hw:dcols].astype(jnp.bfloat16)
        for piece in range(1, per):
            cast(st_g, sb_g, True, piece)
            cast(st_u, sb_u, True, piece)
        for piece in range(per):
            cast(st_d, sb_d, False, piece)
        for index in range(2):
            for piece in range(per):
                a2a_own(index, piece)
        for piece in range(len(parts)):
            a2a_own(2, piece)
    with scope("far_tokens0"):
        tok_arrive(far[0])
        tok_moves(2, start)
    with scope("far_tokens1"):
        tok_arrive(far[1])
        tok_moves(3, start)
    with scope("side_tokens"):
        for m in (1, 3, 5, 7):
            tok_arrive(flip(me, m, groups))
    with scope("arrive_g0"):
        a2a_arrive(0, 0)
        for part in range(3):
            if_edge(lambda: sh_copy(0, me, part).start())
        a2a_start(0, 1)
    with scope("shares"):
        for o in range(1, groups):
            tok_share(1, flip(me, o, groups)).wait_recv()
            tok_share(2, flip(me, o, groups)).start()
        for i in range(2):
            settle(tok.at[pl.ds(0, groups - 1), mine], tok_trecv.at[i])

    def far_shared(k, part):
        sh_copy(0, far[k], part).wait_recv()
        if_inner(lambda: sh_copy(0, far[k], part).start())
        sh_copy(1, far[k], part).start()

    def near_shared():
        for part in range(3):
            sh_copy(0, near, part).wait_recv()
            if part < 2:
                if_inner(lambda: sh_copy(2, near, part).start())
            sh_copy(1, near, part).start()

    def far_shared_start(part):
        for block in (me, near):
            if_inner(lambda: sh_copy(2, block, part).start())

    def shared_sum(part, blocks):
        total = jnp.zeros((tok_count, hcols), jnp.float32)
        for block in blocks:
            columns = pl.ds(pl.multiple_of(block * rows_w, rows_w), rows_w)
            total = total + jnp.dot(
                tok[me, :, columns], sh[block, part], preferred_element_type=jnp.float32
            )
        return total

    def shid_copy(o):
        return tp_copy(
            shid.at[tp], shid.at[tp], shid_send.at[o], shid_recv.at[o], flip(tp, o, ranks)
        )

    def hid_core(e, block):
        return tp_copy(
            hid.at[tp, block, e],
            hid.at[tp, block, e],
            hid_send.at[0],
            hid_recv,
            partner,
        )

    def hid_across(e, block):
        return tp_copy(
            hid.at[tp, block, e],
            hid.at[tp, block, e],
            hid_send.at[1],
            hid_yrecv.at[e, block],
            across,
        )

    def hid_forward(e, block):
        return tp_copy(
            hid.at[across, block, e],
            hid.at[across, block, e],
            hid_send.at[2],
            hid_recv,
            partner,
        )

    def turn(o):
        return (me + o) % groups

    for e in range(per):
        with scope(f"arrive_u{e}"):
            if e == 1:
                a2a_arrive(0, 1)
                a2a_start(2, 0)
            a2a_arrive(1, e)
            if e == 0:
                a2a_start(1, 1)
                for part in range(3):
                    if_inner(lambda: sh_copy(0, me, part).start())
                    sh_copy(1, me, part).start()
                for part in range(2):
                    if_inner(lambda: sh_copy(2, me, part).start())
            else:
                a2a_start(2, 1)
                far_shared_start(2)
                a2a_start(2, 2)
        with scope(f"hidden{e}"):

            @pl.loop(0, groups)
            def _(o):
                block = turn(o + 1)
                rows = tok[block, :, 0:features]
                first = jnp.dot(rows, rv_g[e], preferred_element_type=jnp.float32)
                second = jnp.dot(rows, rv_u[e], preferred_element_type=jnp.float32)
                hid[tp, block, e] = (jax.nn.silu(first) * second).astype(jnp.bfloat16)

                @pl.when(o >= 1)
                def _():
                    before = turn(o)
                    hid_across(e, before).start()
                    hid_core(e, before).start()

            hid_across(e, me).start()
            hid_core(e, me).start()
        if e == 0:
            with scope("near_shared"):
                if_inner(lambda: near_shared())
        with scope(f"forward{e}"):

            @pl.loop(0, groups)
            def _(o):
                block = turn(o + 1)
                hid_across(e, block).wait_recv()
                hid_forward(e, block).start()

        if e == 0:
            with scope("edge_near_shared"):
                if_edge(lambda: near_shared())
            with scope("far_shared_gu"):
                for k in range(2):
                    for part in range(2):
                        far_shared(k, part)

    with scope("hid_wait"):
        settle(hid.at[pl.ds(0, 2)], hid_recv)
        for kind in range(3):
            settle(hid.at[tp], hid_send.at[kind])

    lanes = lax.broadcasted_iota(jnp.int32, (tok_count, LANES), 1)

    def block_out(block, part):
        offset, wide = parts[part]
        table = tok[block, :, features : features + LANES].astype(jnp.float32)
        total = jnp.zeros((tok_count, wide), jnp.float32)
        for e in range(per):
            expert = me * per + e
            weight = jnp.sum(
                jnp.where(
                    (lanes == expert) | (lanes == expert + experts) | (lanes == expert + 2 * experts),
                    table,
                    0.0,
                ),
                axis=1,
                keepdims=True,
            )
            out = jnp.zeros((tok_count, wide), jnp.float32)
            for r in range(ranks):
                out = out + jnp.dot(
                    hid[r, block, e],
                    rv_d[e, r * hcols : (r + 1) * hcols, offset : offset + wide],
                    preferred_element_type=jnp.float32,
                )
            total = total + weight * out
        return total

    def dest(k):
        step = (k + 2 * inn) % 4
        half = z // 2
        away = 1 - step // 2
        chosen = half * (1 - away) + (1 - half) * away
        is_inner = (step % 2) * (1 - away) * inn + (1 - step % 2) * (1 - away) * (1 - inn) + (1 - step % 2) * away
        return chosen * (3 - is_inner) + (1 - chosen) * is_inner

    def x_copy(part, k):
        columns = pl.ds(*parts[part])
        return fs_copy(
            xs.at[k, :, columns], xr.at[k, :, columns], x_send, x_recv.at[part, k], side
        )

    def z_copy(part, k, slot, target):
        columns = pl.ds(*parts[part])
        return fs_copy(
            zs.at[k, :, columns],
            zr.at[slot, :, columns],
            z_send,
            z_recv.at[part, slot],
            target,
        )

    def x_stage(part, pending):
        columns = pl.ds(*parts[part])

        @pl.loop(0, 4)
        def _(k):
            xs[k, :, columns] = block_out(dest(k) * nx + 1 - x, part).astype(jnp.bfloat16)

            if pending is not None:

                @pl.when(k == 0)
                def _():
                    x_copy(pending, 3).start()

            @pl.when(k >= 1)
            def _():
                x_copy(part, k - 1).start()

    def z_stage(part, pending):
        columns = pl.ds(*parts[part])

        @pl.loop(0, 4)
        def _(k):
            total = block_out(dest(k) * nx + x, part)

            if pending is not None:

                @pl.when(k == 0)
                def _():
                    x_copy(pending, 3).start()

            x_copy(part, k).wait_recv()
            total = total + xr[k, :, columns].astype(jnp.float32)
            acc[k, :, columns] = total
            zs[k, :, columns] = total.astype(jnp.bfloat16)

            @pl.when((k >= 1) & edge)
            def _():
                z_copy(part, k - 1, k + 1, near).start()

            @pl.when((k == 1) & inner)
            def _():
                z_copy(part, 0, 4, near).start()

    def z_join(part):
        columns = pl.ds(*parts[part])

        @pl.when(inner)
        def _():
            for k in (2, 3):
                z_copy(part, k, k, near).wait_recv()
                zs[k, :, columns] = (
                    acc[k, :, columns] + zr[k, :, columns].astype(jnp.float32)
                ).astype(jnp.bfloat16)
            own_out[:, columns] = acc[1, :, columns]
            z_copy(part, 2, 5, far_in).start()
            z_copy(part, 3, 5, far_out).start()

        @pl.when(edge)
        def _():
            own_out[:, columns] = acc[3, :, columns]

    def far_shared_d():
        for k in range(2):
            far_shared(k, 2)

    def x_phase(part, pending):
        with scope(f"arrive_d{part}"):
            a2a_arrive(2, part)
        with scope(f"x_stage{part}"):
            x_stage(part, pending)

    def z_phase(part, pending):
        with scope(f"z_stage{part}"):
            z_stage(part, pending)

    def join_phase(part):
        with scope(f"z_join{part}"):
            z_join(part)

    x_phase(0, None)
    x_phase(1, 0)
    z_phase(0, 1)
    with scope("side_shared_gu"):
        for part in range(2):
            for m in (1, 3, 5, 7):
                sh_copy(1, flip(me, m, groups), part).wait_recv()
    with scope("shared_hidden"):
        first, second = (shared_sum(part, range(groups)) for part in range(2))
        shid[tp] = (jax.nn.silu(first) * second).astype(jnp.bfloat16)
        if_inner(lambda: settle(tok.at[pl.ds(0, 3), mine], tok_send.at[0]))
        if_edge(lambda: settle(tok.at[pl.ds(0, 1), mine], tok_send.at[0]))
        settle(tok.at[pl.ds(0, 4), mine], tok_send.at[1])
        if_inner(lambda: settle(tok.at[pl.ds(0, 2), mine], tok_send.at[2]))
        for kind in range(3):
            settle(tok.at[pl.ds(0, groups - 1), mine], tok_tsend.at[kind])
        for o in range(1, ranks):
            shid_copy(o).start()
    with scope("inner_far_shared_d"):
        if_inner(lambda: far_shared_d())
    x_phase(2, None)
    join_phase(0)
    z_phase(1, 2)
    join_phase(1)
    z_phase(2, None)
    with scope("edge_far_shared_d"):
        if_edge(lambda: far_shared_d())
    join_phase(2)
    with scope("side_shared_d"):
        for m in (1, 3, 5, 7):
            sh_copy(1, flip(me, m, groups), 2).wait_recv()
    with scope("drain"):
        for index, sent in enumerate((sb_g, sb_u, sb_d)):
            settle(sent.at[pl.ds(0, experts - per)], a2a_send.at[index])
        if_inner(lambda: settle(sh.at[pl.ds(0, 3)], sh_send.at[0]))
        if_edge(lambda: settle(sh.at[pl.ds(0, 1)], sh_send.at[0]))
        settle(sh.at[pl.ds(0, 4)], sh_send.at[1])
        if_inner(lambda: settle(sh.at[pl.ds(0, 2)], sh_send.at[2]))
        settle(xs, x_send)
        settle(zs.at[pl.ds(0, 3)], z_send)
    with scope("last"):
        for part in range(len(parts)):
            for slot in (4, 5):
                z_copy(part, 0, slot, near).wait_recv()
        for o in range(1, ranks):
            shid_copy(o).wait_recv()
            shid_copy(o).wait_send()


def finish_kernel(
    rv_g, rv_u, rv_d, sh, shid, own_out, zr, gate, up, down, sgate, sup, sdown, mixed, mixed_v, sems
):
    rows_d, hw = sdown.shape[1], sdown.shape[2] // 2
    groups, hcols = sh.shape[0], shid.shape[2]
    moves = [
        (rv_g, gate),
        (rv_u, up),
        (rv_d, down),
        (sh.at[:, 0], sgate),
        (sh.at[:, 1], sup),
        (sh.at[:, 2, pl.ds(0, rows_d)], sdown.at[:, :, pl.ds(0, hw)]),
        (sh.at[:, 2, pl.ds(rows_d, rows_d)], sdown.at[:, :, pl.ds(hw, hw)]),
    ]
    copies = [pltpu.make_async_copy(a, b, sems.at[i]) for i, (a, b) in enumerate(moves)]
    for copy in copies:
        copy.start()
    for part in range(2):
        columns = slice(part * hw, (part + 1) * hw)
        total = own_out[:, columns]
        for slot in (4, 5):
            total = total + zr[slot, :, columns].astype(jnp.float32)
        for block in range(groups):
            at = block * rows_d
            total = total + jnp.dot(
                shid[at // hcols, :, at % hcols : at % hcols + rows_d],
                sh[block, 2, part * rows_d : (part + 1) * rows_d],
                preferred_element_type=jnp.float32,
            )
        mixed_v[:, columns] = total.astype(jnp.bfloat16)
    last = pltpu.make_async_copy(mixed_v, mixed, sems.at[len(moves)])
    last.start()
    for copy in copies:
        copy.wait()
    last.wait()


def dense_body(
    tokens,
    norm_gain,
    expert_gate,
    expert_up,
    expert_down,
    shared_gate,
    shared_up,
    shared_down,
    expert_ids,
    route_weights,
):
    groups, ranks = lax.axis_size("fs"), lax.axis_size("tp")
    experts, rows_w, hcols = expert_gate.shape
    rows_d, dcols = expert_down.shape[1:]
    per = experts // groups
    tok_count, features = tokens.shape
    total = features + LANES
    bf, f32 = jnp.bfloat16, jnp.float32
    dma = pltpu.SemaphoreType.DMA
    any_space = pl.BlockSpec(memory_space=pl.ANY)
    vmem = pl.BlockSpec(memory_space=pltpu.VMEM)
    hidden = hcols * ranks
    wide_rows = -(-tok_count // LANES) * LANES
    made = pl.pallas_call(
        functools.partial(fused_kernel, groups, ranks),
        out_shape=(
            pltpu.VMEM((per, features, hcols), bf),
            pltpu.VMEM((per, features, hcols), bf),
            pltpu.VMEM((per, hidden, dcols), bf),
            pltpu.VMEM((groups, 3, rows_w, hcols), bf),
            pltpu.VMEM((ranks, tok_count, hcols), bf),
            pltpu.VMEM((tok_count, dcols), f32),
            pltpu.VMEM((6, tok_count, dcols), bf),
        ),
        in_specs=[any_space] * 10,
        out_specs=(vmem,) * 7,
        scratch_shapes=[
            pltpu.VMEM((tok_count, features), bf),
            pltpu.VMEM((1, rows_w), f32),
            pltpu.VMEM((TOP_K, tok_count), jnp.int32),
            pltpu.VMEM((TOP_K, tok_count), f32),
            pltpu.VMEM((rows_w, hcols), f32),
            pltpu.VMEM((rows_w, hcols), f32),
            pltpu.VMEM((rows_d, dcols), f32),
            pltpu.VMEM((rows_w, hcols), f32),
            pltpu.VMEM((LANES, wide_rows), f32),
            pltpu.VMEM((experts, rows_w, hcols), f32),
            pltpu.VMEM((experts, rows_w, hcols), f32),
            pltpu.VMEM((experts, rows_d, dcols), f32),
            pltpu.VMEM((experts, rows_w, hcols), bf),
            pltpu.VMEM((experts, rows_w, hcols), bf),
            pltpu.VMEM((experts, rows_d, dcols), bf),
            pltpu.VMEM((groups, tok_count, total), bf),
            pltpu.VMEM((ranks, groups, per, tok_count, hcols), bf),
            pltpu.VMEM((4, tok_count, dcols), bf),
            pltpu.VMEM((4, tok_count, dcols), bf),
            pltpu.VMEM((4, tok_count, dcols), bf),
            pltpu.VMEM((4, tok_count, dcols), f32),
            dma((10,)),
            dma((3,)),
            dma((3, max(per, 3))),
            dma((3,)),
            dma((groups,)),
            dma((3,)),
            dma((2,)),
            dma((groups,)),
            dma((3,)),
            dma((groups, 3)),
            dma((3,)),
            dma,
            dma((per, groups)),
            dma((ranks,)),
            dma((ranks,)),
            dma,
            dma((3, 4)),
            dma,
            dma((3, 6)),
        ],
        compiler_params=pltpu.CompilerParams(
            collective_id=0, has_side_effects=True, vmem_limit_bytes=VMEM_BYTES
        ),
    )(
        tokens,
        norm_gain[None, :],
        expert_ids.T,
        route_weights.T,
        expert_gate,
        expert_up,
        expert_down,
        shared_gate,
        shared_up,
        shared_down,
    )
    gate, up, down, sgate, sup, sdown, mixed = pl.pallas_call(
        finish_kernel,
        out_shape=tuple(
            jax.ShapeDtypeStruct(shape, bf)
            for shape in (
                (per, features, hcols),
                (per, features, hcols),
                (per, hidden, dcols),
                (groups, rows_w, hcols),
                (groups, rows_w, hcols),
                (groups, rows_d, dcols),
                (tok_count, dcols),
            )
        ),
        in_specs=[vmem] * 7,
        out_specs=(any_space,) * 7,
        scratch_shapes=[pltpu.VMEM((tok_count, dcols), bf), dma((8,))],
        compiler_params=pltpu.CompilerParams(vmem_limit_bytes=VMEM_BYTES // 4),
    )(*made)
    return (
        gate,
        up,
        down,
        sgate.reshape(features, hcols),
        sup.reshape(features, hcols),
        sdown.reshape(hidden, dcols),
        mixed,
    )


def expert_hidden(rows, gate_new, up_new):
    first = jnp.einsum("secn,enf->secf", rows, gate_new, preferred_element_type=jnp.float32)
    second = jnp.einsum("secn,enf->secf", rows, up_new, preferred_element_type=jnp.float32)
    return (jax.nn.silu(first) * second).astype(jnp.bfloat16)


def body(
    tokens,
    norm_gain,
    expert_gate,
    expert_up,
    expert_down,
    shared_gate,
    shared_up,
    shared_down,
    expert_ids,
    route_weights,
):
    groups = lax.axis_size("fs")
    experts = expert_gate.shape[0]
    per_group = experts // groups
    tok_count = tokens.shape[0]
    capacity = 2 * tok_count * TOP_K // experts
    ranks = lax.axis_size("tp")
    square = expert_down.shape[1] * expert_down.shape[2] == shared_gate.size
    if capacity >= tok_count and per_group >= 2 and groups == 8 and ranks == 4 and square:
        return dense_body(
            tokens,
            norm_gain,
            expert_gate,
            expert_up,
            expert_down,
            shared_gate,
            shared_up,
            shared_down,
            expert_ids,
            route_weights,
        )
    gate_local = (expert_gate * norm_gain[None, :, None]).astype(jnp.bfloat16)
    up_local = (expert_up * norm_gain[None, :, None]).astype(jnp.bfloat16)
    down_local = expert_down.astype(jnp.bfloat16)
    gate_local = gate_local.reshape((groups, per_group) + gate_local.shape[1:])
    up_local = up_local.reshape((groups, per_group) + up_local.shape[1:])
    down_local = down_local.reshape((groups, per_group) + down_local.shape[1:])
    shared_first_local = (shared_gate * norm_gain[:, None]).astype(jnp.bfloat16)
    shared_second_local = (shared_up * norm_gain[:, None]).astype(jnp.bfloat16)
    shared_third_local = shared_down.astype(jnp.bfloat16)
    gate_moved, up_moved, down_moved = (
        lax.all_to_all(gate_local, "fs", split_axis=0, concat_axis=2, tiled=True),
        lax.all_to_all(up_local, "fs", split_axis=0, concat_axis=2, tiled=True),
        lax.all_to_all(down_local, "fs", split_axis=0, concat_axis=2, tiled=True),
    )
    down_ready = down_moved[0]
    gate_ready = gate_moved[0]
    up_ready = up_moved[0]
    shared_gate_ready, shared_up_ready, shared_down_ready = (
        lax.all_gather(shared_first_local, "fs", axis=0, tiled=True),
        lax.all_gather(shared_second_local, "fs", axis=0, tiled=True),
        lax.all_gather(shared_third_local, "fs", axis=0, tiled=True),
    )
    wide = tokens.astype(jnp.float32)
    normed = (wide * lax.rsqrt(jnp.mean(wide * wide, axis=-1, keepdims=True) + EPS)).astype(
        jnp.bfloat16
    )
    chosen = expert_ids.reshape(-1)
    onehot = (chosen[:, None] == jnp.arange(experts, dtype=jnp.int32)[None, :]).astype(jnp.int32)
    ranks = jnp.sum(jnp.cumsum(onehot, axis=0) * onehot, axis=1) - 1
    owners = jnp.arange(tok_count * TOP_K, dtype=jnp.int32) // TOP_K
    slot_token = jnp.zeros((experts, capacity), jnp.int32).at[chosen, ranks].set(owners)
    outgoing = normed[slot_token.reshape(-1)].reshape(groups, per_group, capacity, normed.shape[1])
    share = capacity // lax.axis_size("tp")
    mine = lax.dynamic_slice_in_dim(outgoing, lax.axis_index("tp") * share, share, 2)
    arrived = lax.all_to_all(mine, "fs", split_axis=0, concat_axis=0, tiled=True)
    hidden = expert_hidden(lax.all_gather(arrived, "tp", axis=2, tiled=True), gate_ready, up_ready)
    shared_first = jnp.dot(normed, shared_gate_ready, preferred_element_type=jnp.float32)
    shared_second = jnp.dot(normed, shared_up_ready, preferred_element_type=jnp.float32)
    shared_hidden = (jax.nn.silu(shared_first) * shared_second).astype(jnp.bfloat16)[None, None]
    columns = down_ready.shape[2]
    routed_piece = lax.all_gather(hidden, "tp", axis=3, tiled=True)
    shared_piece = lax.all_gather(shared_hidden, "tp", axis=3, tiled=True)
    routed_total = jnp.einsum(
        "secf,efd->secd", routed_piece, down_ready, preferred_element_type=jnp.float32
    )
    shared_total = jnp.einsum(
        "abtf,fd->abtd", shared_piece, shared_down_ready, preferred_element_type=jnp.float32
    )
    returned = lax.all_to_all(
        routed_total.astype(jnp.bfloat16), "fs", split_axis=0, concat_axis=0, tiled=True
    )
    returned = returned.reshape(experts * capacity, columns)
    picked = (
        returned[chosen * capacity + ranks].astype(jnp.float32).reshape(tok_count, TOP_K, columns)
    )
    routed = jnp.sum(picked * route_weights[:, :, None], axis=1)
    mixed = (shared_total[0, 0] + routed).astype(jnp.bfloat16)
    return (
        gate_ready,
        up_ready,
        down_ready,
        shared_gate_ready,
        shared_up_ready,
        shared_down_ready,
        mixed,
    )


def solution(mesh):
    in_specs = (
        P("fs", None),
        P("fs"),
        P(None, "fs", "tp"),
        P(None, "fs", "tp"),
        P(None, "fs", "tp"),
        P("fs", "tp"),
        P("fs", "tp"),
        P("fs", "tp"),
        P("fs", None),
        P("fs", None),
    )
    out_specs = (
        P("fs", None, "tp"),
        P("fs", None, "tp"),
        P("fs", None, "tp"),
        P(None, "tp"),
        P(None, "tp"),
        P(None, "tp"),
        P("fs", "tp"),
    )
    return jax.shard_map(body, mesh=mesh, in_specs=in_specs, out_specs=out_specs, check_vma=False)
```

```python
import functools
import jax
import jax.numpy as jnp
from jax import lax
from jax.experimental import pallas as pl
from jax.experimental.pallas import tpu as pltpu
from jax.sharding import PartitionSpec as P

TOP_K = 8


EPS = 1e-06

MESH = pl.DeviceIdType.MESH
LANES = 128
VMEM_BYTES = 44 * 1024 * 1024
scope = jax.named_scope


def flip(value, mask, extent):
    result, bit = 0, 1
    while bit < extent:
        digit = (value // bit) % 2
        result = result + bit * ((1 - digit) if mask & bit else digit)
        bit *= 2
    return result


def fused_kernel(
    groups,
    ranks,
    tokens,
    gain,
    ids,
    weights,
    eg,
    eu,
    ed,
    sg,
    su,
    sd,
    rv_g,
    rv_u,
    rv_d,
    sh,
    shid,
    own_out,
    zr,
    tok_v,
    gain_v,
    ids_v,
    weights_v,
    sg_v,
    su_v,
    sd_v,
    gain_b,
    table_v,
    st_g,
    st_u,
    st_d,
    sb_g,
    sb_u,
    sb_d,
    tok,
    hid,
    xs,
    xr,
    zs,
    acc,
    load_sem,
    a2a_send,
    a2a_recv,
    tok_send,
    tok_recv,
    tok_tsend,
    tok_trecv,
    tok_yrecv,
    sh_send,
    sh_recv,
    hid_send,
    hid_recv,
    hid_yrecv,
    shid_send,
    shid_recv,
    x_send,
    x_recv,
    z_send,
    z_recv,
):
    nx = 2
    me = lax.axis_index("fs")
    tp = lax.axis_index("tp")
    z, x = me // nx, me % nx
    partner = flip(tp, 1, ranks)
    across = flip(tp, 2, ranks)
    per = eg.shape[0] // groups
    experts = eg.shape[0]
    rows_w = eg.shape[1]
    rows_d = ed.shape[1]
    tok_count, features = tokens.shape
    share = tok_count // ranks
    hcols = eg.shape[2]
    dcols = ed.shape[2]
    hw = dcols // 2
    parts = ((0, hw), (hw, hw // 2), (hw + hw // 2, hw // 2))
    inn = ((z + 1) // 2) % 2
    inner, edge = inn == 1, inn == 0
    near, side, far_in, far_out = (flip(me, m, groups) for m in (2, 1, 6, 4))
    far = (inn * far_in + (1 - inn) * far_out, inn * far_out + (1 - inn) * far_in)

    pairs = (
        (gain, gain_v),
        (ids, ids_v),
        (weights, weights_v),
        (tokens, tok_v),
        (eg, st_g),
        (eu, st_u),
        (sg, sg_v),
        (su, su_v),
        (sd, sd_v),
        (ed, st_d),
    )
    loads = [pltpu.make_async_copy(a, b, load_sem.at[i]) for i, (a, b) in enumerate(pairs)]
    for load in loads:
        load.start()

    barrier = pltpu.get_barrier_semaphore()
    for o in range(1, groups):
        pl.semaphore_signal(
            barrier, inc=1, device_id={"fs": flip(me, o, groups)}, device_id_type=MESH
        )
    for o in range(1, ranks):
        pl.semaphore_signal(
            barrier, inc=1, device_id={"tp": flip(tp, o, ranks)}, device_id_type=MESH
        )

    def cast(stage, sendbuf, scaled, piece):
        @pl.loop(0, groups)
        def _(owner):
            e = owner * per + piece
            value = stage[e]
            if scaled:
                value = value * gain_b[...]
            sendbuf[e] = value.astype(jnp.bfloat16)

    mine = pl.ds(tp * share, share)
    theirs = pl.ds(across * share, share)

    def fs_copy(src, dst, send, recv, target):
        return pltpu.make_async_remote_copy(
            src_ref=src,
            dst_ref=dst,
            send_sem=send,
            recv_sem=recv,
            device_id={"fs": target},
            device_id_type=MESH,
        )

    def tp_copy(src, dst, send, recv, target):
        return pltpu.make_async_remote_copy(
            src_ref=src,
            dst_ref=dst,
            send_sem=send,
            recv_sem=recv,
            device_id={"tp": target},
            device_id_type=MESH,
        )

    ways = (near, side, far_in)

    def tok_copy(way, block):
        ref = tok.at[block, mine]
        return fs_copy(ref, ref, tok_send.at[way], tok_recv.at[block], ways[way])

    def sh_copy(way, block, part):
        ref = sh.at[block, part]
        return fs_copy(
            ref, ref, sh_send.at[way], sh_recv.at[block, part], ways[way]
        )

    def if_inner(act):
        pl.when(inner)(act)

    def tok_share(kind, block):
        rows = theirs if kind == 2 else mine
        return tp_copy(
            tok.at[block, rows],
            tok.at[block, rows],
            tok_tsend.at[kind],
            tok_yrecv.at[block] if kind == 1 else tok_trecv.at[kind // 2],
            across if kind == 1 else partner,
        )

    def tok_arrive(block):
        tok_copy(0, block).wait_recv()
        tok_share(0, block).start()
        tok_share(1, block).start()

    def tok_moves(stage, act):
        if stage == 0:
            if_inner(lambda: act(tok_copy(2, me)))
            act(tok_copy(0, me))
            act(tok_copy(1, me))
        elif stage == 1:
            if_inner(lambda: act(tok_copy(2, near)))
            act(tok_copy(1, near))
        else:
            if_inner(lambda: act(tok_copy(0, far[stage - 2])))
            act(tok_copy(1, far[stage - 2]))

    def start(c):
        c.start()

    def wait_send(c):
        c.wait_send()

    order = (6, 7, 4, 5, 2, 3, 1)

    def a2a_ends(index, piece, owner_at, row_at):
        if index < 2:
            sendbuf, recvbuf = ((sb_g, rv_g), (sb_u, rv_u))[index]
            return (
                sendbuf.at[owner_at * per + piece],
                recvbuf.at[piece, pl.ds(row_at * rows_w, rows_w), :],
            )
        columns = pl.ds(*parts[piece])
        return (
            sb_d.at[pl.ds(owner_at * per, per), :, columns],
            rv_d.at[:, pl.ds(row_at * rows_d, rows_d), columns],
        )

    def a2a_copy(index, piece, o):
        target = flip(me, o, groups)
        src, dst = a2a_ends(index, piece, target, me)
        return fs_copy(
            src, dst, a2a_send.at[index], a2a_recv.at[index, piece], target
        )

    def a2a_start(index, piece):
        far_start(index, piece)
        close_start(index, piece)

    def a2a_own(index, piece):
        src, dst = a2a_ends(index, piece, me, me)
        dst[...] = src[...]

    def settle(ref, sem):
        pltpu.make_async_copy(ref, ref, sem).wait()

    def a2a_arrive(index, piece):
        others = groups - 1
        if index < 2:
            ref = (rv_g, rv_u)[index].at[piece, pl.ds(0, others * rows_w)]
        else:
            ref = rv_d.at[:, pl.ds(0, others * rows_d), pl.ds(*parts[piece])]
        settle(ref, a2a_recv.at[index, piece])

    def if_edge(act):
        pl.when(edge)(act)

    def starts(index, piece, targets):
        for o in targets:
            a2a_copy(index, piece, o).start()

    def far_start(index, piece):
        if_inner(lambda: starts(index, piece, (4, 5, 6, 7)))
        if_edge(lambda: starts(index, piece, (6, 7, 4, 5)))

    def close_start(index, piece):
        starts(index, piece, (2, 3, 1))

    with scope("gain"):
        loads[0].wait()
        at_row = lax.broadcasted_iota(jnp.int32, (rows_w, rows_w), 0)
        at_column = lax.broadcasted_iota(jnp.int32, (rows_w, rows_w), 1)
        column = jnp.sum(
            jnp.where(at_row == at_column, gain_v[...], 0.0), axis=1, keepdims=True
        )
        gain_b[...] = jnp.broadcast_to(column, (rows_w, hcols))

    with scope("table"):
        loads[1].wait()
        loads[2].wait()
        row = lax.broadcasted_iota(jnp.int32, (experts, tok_count), 0)
        table = jnp.zeros((experts, tok_count), jnp.float32)
        for k in range(ids.shape[0]):
            table = table + jnp.where(row == ids_v[k : k + 1, :], weights_v[k : k + 1, :], 0.0)
        high = table.astype(jnp.bfloat16).astype(jnp.float32)
        middle = (table - high).astype(jnp.bfloat16).astype(jnp.float32)
        table_v[...] = jnp.zeros(table_v.shape, jnp.float32)
        for i, value in enumerate((high, middle, table - high - middle)):
            table_v[i * experts : (i + 1) * experts, 0:tok_count] = value
        tok[me, :, features : features + LANES] = table_v[...].T[0:tok_count].astype(jnp.bfloat16)

    def norm(first, count):
        @pl.loop(0, count // 16)
        def _(i):
            rows = pl.ds(first + i * 16, 16)
            wide = tok_v[rows, :].astype(jnp.float32)
            mean = jnp.mean(wide * wide, axis=-1, keepdims=True)
            tok[me, rows, 0:features] = (wide * lax.rsqrt(mean + EPS)).astype(jnp.bfloat16)

    with scope("norm"):
        loads[3].wait()
        norm(tp * share, share)

    with scope("barrier"):
        pl.semaphore_wait(barrier, groups + ranks - 2)

    with scope("launch"):
        tok_moves(0, start)
        loads[4].wait()
        cast(st_g, sb_g, True, 0)

        if_edge(lambda: starts(0, 0, (6, 7, 4, 5)))
        close_start(0, 0)
        for o in range(1, ranks):
            norm(flip(tp, o, ranks) * share, share)
        loads[5].wait()
        cast(st_u, sb_u, True, 0)
    with scope("near_tokens"):
        tok_arrive(near)
        tok_moves(1, start)

        if_inner(lambda: starts(0, 0, (4, 5, 6, 7)))
        far_start(1, 0)
        close_start(1, 0)
    with scope("casts"):
        for i in range(6, 10):
            loads[i].wait()
        sh[me, 0] = (sg_v[...] * gain_b[...]).astype(jnp.bfloat16)
        sh[me, 1] = (su_v[...] * gain_b[...]).astype(jnp.bfloat16)
        sh[me, 2, 0:rows_d] = sd_v[:, 0:hw].astype(jnp.bfloat16)
        sh[me, 2, rows_d : 2 * rows_d] = sd_v[:, hw:dcols].astype(jnp.bfloat16)
        for piece in range(1, per):
            cast(st_g, sb_g, True, piece)
            cast(st_u, sb_u, True, piece)
        for piece in range(per):
            cast(st_d, sb_d, False, piece)
        for index in range(2):
            for piece in range(per):
                a2a_own(index, piece)
        for piece in range(len(parts)):
            a2a_own(2, piece)
    with scope("far_tokens0"):
        tok_arrive(far[0])
        tok_moves(2, start)
    with scope("far_tokens1"):
        tok_arrive(far[1])
        tok_moves(3, start)
    with scope("side_tokens"):
        for m in (1, 3, 5, 7):
            tok_arrive(flip(me, m, groups))
    with scope("arrive_g0"):
        a2a_arrive(0, 0)
        for part in range(3):
            if_edge(lambda: sh_copy(0, me, part).start())
        a2a_start(0, 1)
    with scope("shares"):
        for o in range(1, groups):
            tok_share(1, flip(me, o, groups)).wait_recv()
            tok_share(2, flip(me, o, groups)).start()
        for i in range(2):
            settle(tok.at[pl.ds(0, groups - 1), mine], tok_trecv.at[i])

    def far_shared(k, part):
        sh_copy(0, far[k], part).wait_recv()
        if_inner(lambda: sh_copy(0, far[k], part).start())
        sh_copy(1, far[k], part).start()

    def near_shared():
        for part in range(3):
            sh_copy(0, near, part).wait_recv()
            if part < 2:
                if_inner(lambda: sh_copy(2, near, part).start())
            sh_copy(1, near, part).start()

    def far_shared_start(part):
        for block in (me, near):
            if_inner(lambda: sh_copy(2, block, part).start())

    def shared_sum(part, blocks):
        total = jnp.zeros((tok_count, hcols), jnp.float32)
        for block in blocks:
            columns = pl.ds(pl.multiple_of(block * rows_w, rows_w), rows_w)
            total = total + jnp.dot(
                tok[me, :, columns], sh[block, part], preferred_element_type=jnp.float32
            )
        return total

    def shid_copy(o):
        return tp_copy(
            shid.at[tp], shid.at[tp], shid_send.at[o], shid_recv.at[o], flip(tp, o, ranks)
        )

    def hid_core(e, block):
        return tp_copy(
            hid.at[tp, block, e],
            hid.at[tp, block, e],
            hid_send.at[0],
            hid_recv,
            partner,
        )

    def hid_across(e, block):
        return tp_copy(
            hid.at[tp, block, e],
            hid.at[tp, block, e],
            hid_send.at[1],
            hid_yrecv.at[e, block],
            across,
        )

    def hid_forward(e, block):
        return tp_copy(
            hid.at[across, block, e],
            hid.at[across, block, e],
            hid_send.at[2],
            hid_recv,
            partner,
        )

    def turn(o):
        return (me + o) % groups

    for e in range(per):
        with scope(f"arrive_u{e}"):
            if e == 1:

                @pl.when(edge)
                def _():
                    a2a_arrive(0, 1)
                    starts(2, 0, (6, 7, 4, 5))

                close_start(2, 0)
            a2a_arrive(1, e)
            if e == 0:
                a2a_start(1, 1)
                for part in range(3):
                    if_inner(lambda: sh_copy(0, me, part).start())
                    sh_copy(1, me, part).start()
                for part in range(2):
                    if_inner(lambda: sh_copy(2, me, part).start())
            else:
                a2a_start(2, 1)
                far_shared_start(2)
                a2a_start(2, 2)
        with scope(f"hidden{e}"):

            @pl.loop(0, groups)
            def _(o):
                block = turn(o + 1)
                rows = tok[block, :, 0:features]
                first = jnp.dot(rows, rv_g[e], preferred_element_type=jnp.float32)
                second = jnp.dot(rows, rv_u[e], preferred_element_type=jnp.float32)
                hid[tp, block, e] = (jax.nn.silu(first) * second).astype(jnp.bfloat16)

                @pl.when(o >= 1)
                def _():
                    before = turn(o)
                    hid_across(e, before).start()
                    hid_core(e, before).start()

            hid_across(e, me).start()
            hid_core(e, me).start()
        if e == 0:
            with scope("near_shared"):
                if_inner(lambda: near_shared())
        with scope(f"forward{e}"):

            @pl.loop(0, groups)
            def _(o):
                block = turn(o + 1)
                hid_across(e, block).wait_recv()
                hid_forward(e, block).start()

        if e == 0:
            with scope("edge_near_shared"):
                if_edge(lambda: near_shared())
            with scope("far_shared_gu"):
                for k, part in ((0, 0), (0, 1), (1, 0)):
                    far_shared(k, part)

                @pl.when(inner)
                def _():
                    a2a_arrive(0, 1)
                    starts(2, 0, (4, 5, 6, 7))

                far_shared(1, 1)

    with scope("hid_wait"):
        settle(hid.at[pl.ds(0, 2)], hid_recv)
        for kind in range(3):
            settle(hid.at[tp], hid_send.at[kind])

    lanes = lax.broadcasted_iota(jnp.int32, (tok_count, LANES), 1)

    def block_out(block, part):
        offset, wide = parts[part]
        table = tok[block, :, features : features + LANES].astype(jnp.float32)
        total = jnp.zeros((tok_count, wide), jnp.float32)
        for e in range(per):
            expert = me * per + e
            weight = jnp.sum(
                jnp.where(
                    (lanes == expert) | (lanes == expert + experts) | (lanes == expert + 2 * experts),
                    table,
                    0.0,
                ),
                axis=1,
                keepdims=True,
            )
            out = jnp.zeros((tok_count, wide), jnp.float32)
            for r in range(ranks):
                out = out + jnp.dot(
                    hid[r, block, e],
                    rv_d[e, r * hcols : (r + 1) * hcols, offset : offset + wide],
                    preferred_element_type=jnp.float32,
                )
            total = total + weight * out
        return total

    def dest(k):
        step = (k + 2 * inn) % 4
        half = z // 2
        away = 1 - step // 2
        chosen = half * (1 - away) + (1 - half) * away
        is_inner = (step % 2) * (1 - away) * inn + (1 - step % 2) * (1 - away) * (1 - inn) + (1 - step % 2) * away
        return chosen * (3 - is_inner) + (1 - chosen) * is_inner

    def x_copy(part, k):
        columns = pl.ds(*parts[part])
        return fs_copy(
            xs.at[k, :, columns], xr.at[k, :, columns], x_send, x_recv.at[part, k], side
        )

    def z_copy(part, k, slot, target):
        columns = pl.ds(*parts[part])
        return fs_copy(
            zs.at[k, :, columns],
            zr.at[slot, :, columns],
            z_send,
            z_recv.at[part, slot],
            target,
        )

    def x_stage(part, pending):
        columns = pl.ds(*parts[part])

        @pl.loop(0, 4)
        def _(k):
            xs[k, :, columns] = block_out(dest(k) * nx + 1 - x, part).astype(jnp.bfloat16)

            if pending is not None:

                @pl.when(k == 0)
                def _():
                    x_copy(pending, 3).start()

            @pl.when(k >= 1)
            def _():
                x_copy(part, k - 1).start()

    def z_stage(part, pending):
        columns = pl.ds(*parts[part])

        @pl.loop(0, 4)
        def _(k):
            total = block_out(dest(k) * nx + x, part)

            if pending is not None:

                @pl.when(k == 0)
                def _():
                    x_copy(pending, 3).start()

            x_copy(part, k).wait_recv()
            total = total + xr[k, :, columns].astype(jnp.float32)
            acc[k, :, columns] = total
            zs[k, :, columns] = total.astype(jnp.bfloat16)

            @pl.when((k >= 1) & edge)
            def _():
                z_copy(part, k - 1, k + 1, near).start()

            @pl.when((k == 1) & inner)
            def _():
                z_copy(part, 0, 4, near).start()

    def z_join(part):
        columns = pl.ds(*parts[part])

        @pl.when(inner)
        def _():
            for k in (2, 3):
                z_copy(part, k, k, near).wait_recv()
                zs[k, :, columns] = (
                    acc[k, :, columns] + zr[k, :, columns].astype(jnp.float32)
                ).astype(jnp.bfloat16)
            own_out[:, columns] = acc[1, :, columns]
            z_copy(part, 2, 5, far_in).start()
            z_copy(part, 3, 5, far_out).start()

        @pl.when(edge)
        def _():
            own_out[:, columns] = acc[3, :, columns]

    def far_shared_d():
        for k in range(2):
            far_shared(k, 2)

    def x_phase(part, pending):
        with scope(f"arrive_d{part}"):
            a2a_arrive(2, part)
        with scope(f"x_stage{part}"):
            x_stage(part, pending)

    def z_phase(part, pending):
        with scope(f"z_stage{part}"):
            z_stage(part, pending)

    def join_phase(part):
        with scope(f"z_join{part}"):
            z_join(part)

    x_phase(0, None)
    x_phase(1, 0)
    z_phase(0, 1)
    with scope("side_shared_gu"):
        for part in range(2):
            for m in (1, 3, 5, 7):
                sh_copy(1, flip(me, m, groups), part).wait_recv()
    with scope("shared_hidden"):
        first, second = (shared_sum(part, range(groups)) for part in range(2))
        shid[tp] = (jax.nn.silu(first) * second).astype(jnp.bfloat16)
        if_inner(lambda: settle(tok.at[pl.ds(0, 3), mine], tok_send.at[0]))
        if_edge(lambda: settle(tok.at[pl.ds(0, 1), mine], tok_send.at[0]))
        settle(tok.at[pl.ds(0, 4), mine], tok_send.at[1])
        if_inner(lambda: settle(tok.at[pl.ds(0, 2), mine], tok_send.at[2]))
        for kind in range(3):
            settle(tok.at[pl.ds(0, groups - 1), mine], tok_tsend.at[kind])
        for o in range(1, ranks):
            shid_copy(o).start()
    with scope("inner_far_shared_d"):
        if_inner(lambda: far_shared_d())
    z_phase(1, None)
    with scope("arrive_d2"):
        a2a_arrive(2, 2)
    join_phase(0)
    join_phase(1)
    with scope("x_stage2"):
        x_stage(2, None)
    z_phase(2, 2)
    with scope("edge_far_shared_d"):
        if_edge(lambda: far_shared_d())
    join_phase(2)
    with scope("side_shared_d"):
        for m in (1, 3, 5, 7):
            sh_copy(1, flip(me, m, groups), 2).wait_recv()
    with scope("drain"):
        for index, sent in enumerate((sb_g, sb_u, sb_d)):
            settle(sent.at[pl.ds(0, experts - per)], a2a_send.at[index])
        if_inner(lambda: settle(sh.at[pl.ds(0, 3)], sh_send.at[0]))
        if_edge(lambda: settle(sh.at[pl.ds(0, 1)], sh_send.at[0]))
        settle(sh.at[pl.ds(0, 4)], sh_send.at[1])
        if_inner(lambda: settle(sh.at[pl.ds(0, 2)], sh_send.at[2]))
        settle(xs, x_send)
        settle(zs.at[pl.ds(0, 3)], z_send)
    with scope("last"):
        for part in range(len(parts)):
            for slot in (4, 5):
                z_copy(part, 0, slot, near).wait_recv()
        for o in range(1, ranks):
            shid_copy(o).wait_recv()
            shid_copy(o).wait_send()


def finish_kernel(
    rv_g, rv_u, rv_d, sh, shid, own_out, zr, gate, up, down, sgate, sup, sdown, mixed, mixed_v, sems
):
    rows_d, hw = sdown.shape[1], sdown.shape[2] // 2
    groups, hcols = sh.shape[0], shid.shape[2]
    moves = [
        (rv_g, gate),
        (rv_u, up),
        (rv_d, down),
        (sh.at[:, 0], sgate),
        (sh.at[:, 1], sup),
        (sh.at[:, 2, pl.ds(0, rows_d)], sdown.at[:, :, pl.ds(0, hw)]),
        (sh.at[:, 2, pl.ds(rows_d, rows_d)], sdown.at[:, :, pl.ds(hw, hw)]),
    ]
    copies = [pltpu.make_async_copy(a, b, sems.at[i]) for i, (a, b) in enumerate(moves)]
    for copy in copies:
        copy.start()
    for part in range(2):
        columns = slice(part * hw, (part + 1) * hw)
        total = own_out[:, columns]
        for slot in (4, 5):
            total = total + zr[slot, :, columns].astype(jnp.float32)
        for block in range(groups):
            at = block * rows_d
            total = total + jnp.dot(
                shid[at // hcols, :, at % hcols : at % hcols + rows_d],
                sh[block, 2, part * rows_d : (part + 1) * rows_d],
                preferred_element_type=jnp.float32,
            )
        mixed_v[:, columns] = total.astype(jnp.bfloat16)
    last = pltpu.make_async_copy(mixed_v, mixed, sems.at[len(moves)])
    last.start()
    for copy in copies:
        copy.wait()
    last.wait()


def dense_body(
    tokens,
    norm_gain,
    expert_gate,
    expert_up,
    expert_down,
    shared_gate,
    shared_up,
    shared_down,
    expert_ids,
    route_weights,
):
    groups, ranks = lax.axis_size("fs"), lax.axis_size("tp")
    experts, rows_w, hcols = expert_gate.shape
    rows_d, dcols = expert_down.shape[1:]
    per = experts // groups
    tok_count, features = tokens.shape
    total = features + LANES
    bf, f32 = jnp.bfloat16, jnp.float32
    dma = pltpu.SemaphoreType.DMA
    any_space = pl.BlockSpec(memory_space=pl.ANY)
    vmem = pl.BlockSpec(memory_space=pltpu.VMEM)
    hidden = hcols * ranks
    wide_rows = -(-tok_count // LANES) * LANES
    made = pl.pallas_call(
        functools.partial(fused_kernel, groups, ranks),
        out_shape=(
            pltpu.VMEM((per, features, hcols), bf),
            pltpu.VMEM((per, features, hcols), bf),
            pltpu.VMEM((per, hidden, dcols), bf),
            pltpu.VMEM((groups, 3, rows_w, hcols), bf),
            pltpu.VMEM((ranks, tok_count, hcols), bf),
            pltpu.VMEM((tok_count, dcols), f32),
            pltpu.VMEM((6, tok_count, dcols), bf),
        ),
        in_specs=[any_space] * 10,
        out_specs=(vmem,) * 7,
        scratch_shapes=[
            pltpu.VMEM((tok_count, features), bf),
            pltpu.VMEM((1, rows_w), f32),
            pltpu.VMEM((TOP_K, tok_count), jnp.int32),
            pltpu.VMEM((TOP_K, tok_count), f32),
            pltpu.VMEM((rows_w, hcols), f32),
            pltpu.VMEM((rows_w, hcols), f32),
            pltpu.VMEM((rows_d, dcols), f32),
            pltpu.VMEM((rows_w, hcols), f32),
            pltpu.VMEM((LANES, wide_rows), f32),
            pltpu.VMEM((experts, rows_w, hcols), f32),
            pltpu.VMEM((experts, rows_w, hcols), f32),
            pltpu.VMEM((experts, rows_d, dcols), f32),
            pltpu.VMEM((experts, rows_w, hcols), bf),
            pltpu.VMEM((experts, rows_w, hcols), bf),
            pltpu.VMEM((experts, rows_d, dcols), bf),
            pltpu.VMEM((groups, tok_count, total), bf),
            pltpu.VMEM((ranks, groups, per, tok_count, hcols), bf),
            pltpu.VMEM((4, tok_count, dcols), bf),
            pltpu.VMEM((4, tok_count, dcols), bf),
            pltpu.VMEM((4, tok_count, dcols), bf),
            pltpu.VMEM((4, tok_count, dcols), f32),
            dma((10,)),
            dma((3,)),
            dma((3, max(per, 3))),
            dma((3,)),
            dma((groups,)),
            dma((3,)),
            dma((2,)),
            dma((groups,)),
            dma((3,)),
            dma((groups, 3)),
            dma((3,)),
            dma,
            dma((per, groups)),
            dma((ranks,)),
            dma((ranks,)),
            dma,
            dma((3, 4)),
            dma,
            dma((3, 6)),
        ],
        compiler_params=pltpu.CompilerParams(
            collective_id=0, has_side_effects=True, vmem_limit_bytes=VMEM_BYTES
        ),
    )(
        tokens,
        norm_gain[None, :],
        expert_ids.T,
        route_weights.T,
        expert_gate,
        expert_up,
        expert_down,
        shared_gate,
        shared_up,
        shared_down,
    )
    gate, up, down, sgate, sup, sdown, mixed = pl.pallas_call(
        finish_kernel,
        out_shape=tuple(
            jax.ShapeDtypeStruct(shape, bf)
            for shape in (
                (per, features, hcols),
                (per, features, hcols),
                (per, hidden, dcols),
                (groups, rows_w, hcols),
                (groups, rows_w, hcols),
                (groups, rows_d, dcols),
                (tok_count, dcols),
            )
        ),
        in_specs=[vmem] * 7,
        out_specs=(any_space,) * 7,
        scratch_shapes=[pltpu.VMEM((tok_count, dcols), bf), dma((8,))],
        compiler_params=pltpu.CompilerParams(vmem_limit_bytes=VMEM_BYTES // 4),
    )(*made)
    return (
        gate,
        up,
        down,
        sgate.reshape(features, hcols),
        sup.reshape(features, hcols),
        sdown.reshape(hidden, dcols),
        mixed,
    )


def expert_hidden(rows, gate_new, up_new):
    first = jnp.einsum("secn,enf->secf", rows, gate_new, preferred_element_type=jnp.float32)
    second = jnp.einsum("secn,enf->secf", rows, up_new, preferred_element_type=jnp.float32)
    return (jax.nn.silu(first) * second).astype(jnp.bfloat16)


def body(
    tokens,
    norm_gain,
    expert_gate,
    expert_up,
    expert_down,
    shared_gate,
    shared_up,
    shared_down,
    expert_ids,
    route_weights,
):
    groups = lax.axis_size("fs")
    experts = expert_gate.shape[0]
    per_group = experts // groups
    tok_count = tokens.shape[0]
    capacity = 2 * tok_count * TOP_K // experts
    ranks = lax.axis_size("tp")
    square = expert_down.shape[1] * expert_down.shape[2] == shared_gate.size
    if capacity >= tok_count and per_group >= 2 and groups == 8 and ranks == 4 and square:
        return dense_body(
            tokens,
            norm_gain,
            expert_gate,
            expert_up,
            expert_down,
            shared_gate,
            shared_up,
            shared_down,
            expert_ids,
            route_weights,
        )
    gate_local = (expert_gate * norm_gain[None, :, None]).astype(jnp.bfloat16)
    up_local = (expert_up * norm_gain[None, :, None]).astype(jnp.bfloat16)
    down_local = expert_down.astype(jnp.bfloat16)
    gate_local = gate_local.reshape((groups, per_group) + gate_local.shape[1:])
    up_local = up_local.reshape((groups, per_group) + up_local.shape[1:])
    down_local = down_local.reshape((groups, per_group) + down_local.shape[1:])
    shared_first_local = (shared_gate * norm_gain[:, None]).astype(jnp.bfloat16)
    shared_second_local = (shared_up * norm_gain[:, None]).astype(jnp.bfloat16)
    shared_third_local = shared_down.astype(jnp.bfloat16)
    gate_moved, up_moved, down_moved = (
        lax.all_to_all(gate_local, "fs", split_axis=0, concat_axis=2, tiled=True),
        lax.all_to_all(up_local, "fs", split_axis=0, concat_axis=2, tiled=True),
        lax.all_to_all(down_local, "fs", split_axis=0, concat_axis=2, tiled=True),
    )
    down_ready = down_moved[0]
    gate_ready = gate_moved[0]
    up_ready = up_moved[0]
    shared_gate_ready, shared_up_ready, shared_down_ready = (
        lax.all_gather(shared_first_local, "fs", axis=0, tiled=True),
        lax.all_gather(shared_second_local, "fs", axis=0, tiled=True),
        lax.all_gather(shared_third_local, "fs", axis=0, tiled=True),
    )
    wide = tokens.astype(jnp.float32)
    normed = (wide * lax.rsqrt(jnp.mean(wide * wide, axis=-1, keepdims=True) + EPS)).astype(
        jnp.bfloat16
    )
    chosen = expert_ids.reshape(-1)
    onehot = (chosen[:, None] == jnp.arange(experts, dtype=jnp.int32)[None, :]).astype(jnp.int32)
    ranks = jnp.sum(jnp.cumsum(onehot, axis=0) * onehot, axis=1) - 1
    owners = jnp.arange(tok_count * TOP_K, dtype=jnp.int32) // TOP_K
    slot_token = jnp.zeros((experts, capacity), jnp.int32).at[chosen, ranks].set(owners)
    outgoing = normed[slot_token.reshape(-1)].reshape(groups, per_group, capacity, normed.shape[1])
    share = capacity // lax.axis_size("tp")
    mine = lax.dynamic_slice_in_dim(outgoing, lax.axis_index("tp") * share, share, 2)
    arrived = lax.all_to_all(mine, "fs", split_axis=0, concat_axis=0, tiled=True)
    hidden = expert_hidden(lax.all_gather(arrived, "tp", axis=2, tiled=True), gate_ready, up_ready)
    shared_first = jnp.dot(normed, shared_gate_ready, preferred_element_type=jnp.float32)
    shared_second = jnp.dot(normed, shared_up_ready, preferred_element_type=jnp.float32)
    shared_hidden = (jax.nn.silu(shared_first) * shared_second).astype(jnp.bfloat16)[None, None]
    columns = down_ready.shape[2]
    routed_piece = lax.all_gather(hidden, "tp", axis=3, tiled=True)
    shared_piece = lax.all_gather(shared_hidden, "tp", axis=3, tiled=True)
    routed_total = jnp.einsum(
        "secf,efd->secd", routed_piece, down_ready, preferred_element_type=jnp.float32
    )
    shared_total = jnp.einsum(
        "abtf,fd->abtd", shared_piece, shared_down_ready, preferred_element_type=jnp.float32
    )
    returned = lax.all_to_all(
        routed_total.astype(jnp.bfloat16), "fs", split_axis=0, concat_axis=0, tiled=True
    )
    returned = returned.reshape(experts * capacity, columns)
    picked = (
        returned[chosen * capacity + ranks].astype(jnp.float32).reshape(tok_count, TOP_K, columns)
    )
    routed = jnp.sum(picked * route_weights[:, :, None], axis=1)
    mixed = (shared_total[0, 0] + routed).astype(jnp.bfloat16)
    return (
        gate_ready,
        up_ready,
        down_ready,
        shared_gate_ready,
        shared_up_ready,
        shared_down_ready,
        mixed,
    )


def solution(mesh):
    in_specs = (
        P("fs", None),
        P("fs"),
        P(None, "fs", "tp"),
        P(None, "fs", "tp"),
        P(None, "fs", "tp"),
        P("fs", "tp"),
        P("fs", "tp"),
        P("fs", "tp"),
        P("fs", None),
        P("fs", None),
    )
    out_specs = (
        P("fs", None, "tp"),
        P("fs", None, "tp"),
        P("fs", None, "tp"),
        P(None, "tp"),
        P(None, "tp"),
        P(None, "tp"),
        P("fs", "tp"),
    )
    return jax.shard_map(body, mesh=mesh, in_specs=in_specs, out_specs=out_specs, check_vma=False)
```

```python
import functools
import jax
import jax.numpy as jnp
from jax import lax
from jax.experimental import pallas as pl
from jax.experimental.pallas import tpu as pltpu
from jax.sharding import PartitionSpec as P

TOP_K = 8


EPS = 1e-06

MESH = pl.DeviceIdType.MESH
LANES = 128
VMEM_BYTES = 44 * 1024 * 1024
scope = jax.named_scope


def flip(value, mask, extent):
    result, bit = 0, 1
    while bit < extent:
        digit = (value // bit) % 2
        result = result + bit * ((1 - digit) if mask & bit else digit)
        bit *= 2
    return result


def fused_kernel(
    groups,
    ranks,
    tokens,
    gain,
    ids,
    weights,
    eg,
    eu,
    ed,
    sg,
    su,
    sd,
    rv_g,
    rv_u,
    rv_d,
    sh,
    shid,
    own_out,
    zr,
    tok_v,
    gain_v,
    ids_v,
    weights_v,
    sg_v,
    su_v,
    sd_v,
    gain_b,
    table_v,
    st_g,
    st_u,
    st_d,
    sb_g,
    sb_u,
    sb_d,
    tok,
    hid,
    xs,
    xr,
    zs,
    acc,
    load_sem,
    a2a_send,
    a2a_recv,
    tok_send,
    tok_recv,
    tok_tsend,
    tok_trecv,
    tok_yrecv,
    sh_send,
    sh_recv,
    sh_srecv,
    hid_send,
    hid_recv,
    hid_yrecv,
    shid_send,
    shid_recv,
    x_send,
    x_recv,
    z_send,
    z_recv,
    z_last,
):
    nx = 2
    me = lax.axis_index("fs")
    tp = lax.axis_index("tp")
    z, x = me // nx, me % nx
    partner = flip(tp, 1, ranks)
    across = flip(tp, 2, ranks)
    per = eg.shape[0] // groups
    experts = eg.shape[0]
    rows_w = eg.shape[1]
    rows_d = ed.shape[1]
    tok_count, features = tokens.shape
    share = tok_count // ranks
    hcols = eg.shape[2]
    dcols = ed.shape[2]
    hw = dcols // 2
    parts = ((0, hw), (hw, hw // 2), (hw + hw // 2, hw // 2))
    inn = ((z + 1) // 2) % 2
    inner, edge = inn == 1, inn == 0
    near, side, far_in, far_out = (flip(me, m, groups) for m in (2, 1, 6, 4))
    far = (inn * far_in + (1 - inn) * far_out, inn * far_out + (1 - inn) * far_in)

    pairs = (
        (gain, gain_v),
        (ids, ids_v),
        (weights, weights_v),
        (tokens, tok_v),
        (eg, st_g),
        (eu, st_u),
        (sg, sg_v),
        (su, su_v),
        (sd, sd_v),
        (ed, st_d),
    )
    loads = [pltpu.make_async_copy(a, b, load_sem.at[i]) for i, (a, b) in enumerate(pairs)]
    for load in loads:
        load.start()

    barrier = pltpu.get_barrier_semaphore()
    for o in range(1, groups):
        pl.semaphore_signal(
            barrier, inc=1, device_id={"fs": flip(me, o, groups)}, device_id_type=MESH
        )
    for o in range(1, ranks):
        pl.semaphore_signal(
            barrier, inc=1, device_id={"tp": flip(tp, o, ranks)}, device_id_type=MESH
        )

    def cast(stage, sendbuf, scaled, piece):
        @pl.loop(0, groups)
        def _(owner):
            e = owner * per + piece
            value = stage[e]
            if scaled:
                value = value * gain_b[...]
            sendbuf[e] = value.astype(jnp.bfloat16)

    mine = pl.ds(tp * share, share)
    theirs = pl.ds(across * share, share)

    def fs_copy(src, dst, send, recv, target):
        return pltpu.make_async_remote_copy(
            src_ref=src,
            dst_ref=dst,
            send_sem=send,
            recv_sem=recv,
            device_id={"fs": target},
            device_id_type=MESH,
        )

    def tp_copy(src, dst, send, recv, target):
        return pltpu.make_async_remote_copy(
            src_ref=src,
            dst_ref=dst,
            send_sem=send,
            recv_sem=recv,
            device_id={"tp": target},
            device_id_type=MESH,
        )

    ways = (near, side, far_in)

    def tok_copy(way, block):
        ref = tok.at[block, mine]
        return fs_copy(ref, ref, tok_send.at[way], tok_recv.at[block], ways[way])

    def sh_copy(way, block, part):
        ref = sh.at[block, part]
        return fs_copy(
            ref,
            ref,
            sh_send.at[way],
            sh_srecv.at[part // 2] if way == 1 else sh_recv.at[block // nx, part],
            ways[way],
        )

    def if_inner(act):
        pl.when(inner)(act)

    def tok_share(kind, block):
        rows = theirs if kind == 2 else mine
        return tp_copy(
            tok.at[block, rows],
            tok.at[block, rows],
            tok_tsend.at[kind],
            tok_yrecv.at[block] if kind == 1 else tok_trecv.at[kind // 2],
            across if kind == 1 else partner,
        )

    def tok_arrive(block):
        tok_copy(0, block).wait_recv()
        tok_share(0, block).start()
        tok_share(1, block).start()

    def tok_moves(stage, act):
        if stage == 0:
            if_inner(lambda: act(tok_copy(2, me)))
            act(tok_copy(0, me))
            act(tok_copy(1, me))
        elif stage == 1:
            if_inner(lambda: act(tok_copy(2, near)))
            act(tok_copy(1, near))
        else:
            if_inner(lambda: act(tok_copy(0, far[stage - 2])))
            act(tok_copy(1, far[stage - 2]))

    def start(c):
        c.start()

    def wait_send(c):
        c.wait_send()

    order = (6, 7, 4, 5, 2, 3, 1)

    def a2a_ends(index, piece, owner_at, row_at):
        if index < 2:
            sendbuf, recvbuf = ((sb_g, rv_g), (sb_u, rv_u))[index]
            return (
                sendbuf.at[owner_at * per + piece],
                recvbuf.at[piece, pl.ds(row_at * rows_w, rows_w), :],
            )
        columns = pl.ds(*parts[piece])
        return (
            sb_d.at[pl.ds(owner_at * per, per), :, columns],
            rv_d.at[:, pl.ds(row_at * rows_d, rows_d), columns],
        )

    def a2a_copy(index, piece, o):
        target = flip(me, o, groups)
        src, dst = a2a_ends(index, piece, target, me)
        return fs_copy(
            src, dst, a2a_send.at[index], a2a_recv.at[index, piece], target
        )

    def a2a_start(index, piece):
        far_start(index, piece)
        close_start(index, piece)

    def a2a_own(index, piece):
        src, dst = a2a_ends(index, piece, me, me)
        dst[...] = src[...]

    def settle(ref, sem):
        pltpu.make_async_copy(ref, ref, sem).wait()

    def a2a_arrive(index, piece):
        others = groups - 1
        if index < 2:
            ref = (rv_g, rv_u)[index].at[piece, pl.ds(0, others * rows_w)]
        else:
            ref = rv_d.at[:, pl.ds(0, others * rows_d), pl.ds(*parts[piece])]
        settle(ref, a2a_recv.at[index, piece])

    def if_edge(act):
        pl.when(edge)(act)

    def starts(index, piece, targets):
        for o in targets:
            a2a_copy(index, piece, o).start()

    def far_start(index, piece):
        if_inner(lambda: starts(index, piece, (4, 5, 6, 7)))
        if_edge(lambda: starts(index, piece, (6, 7, 4, 5)))

    def close_start(index, piece):
        starts(index, piece, (2, 3, 1))

    with scope("gain"):
        loads[0].wait()
        at_row = lax.broadcasted_iota(jnp.int32, (rows_w, rows_w), 0)
        at_column = lax.broadcasted_iota(jnp.int32, (rows_w, rows_w), 1)
        column = jnp.sum(
            jnp.where(at_row == at_column, gain_v[...], 0.0), axis=1, keepdims=True
        )
        gain_b[...] = jnp.broadcast_to(column, (rows_w, hcols))

    with scope("table"):
        loads[1].wait()
        loads[2].wait()
        row = lax.broadcasted_iota(jnp.int32, (experts, tok_count), 0)
        table = jnp.zeros((experts, tok_count), jnp.float32)
        for k in range(ids.shape[0]):
            table = table + jnp.where(row == ids_v[k : k + 1, :], weights_v[k : k + 1, :], 0.0)
        high = table.astype(jnp.bfloat16).astype(jnp.float32)
        middle = (table - high).astype(jnp.bfloat16).astype(jnp.float32)
        table_v[...] = jnp.zeros(table_v.shape, jnp.float32)
        for i, value in enumerate((high, middle, table - high - middle)):
            table_v[i * experts : (i + 1) * experts, 0:tok_count] = value
        tok[me, :, features : features + LANES] = table_v[...].T[0:tok_count].astype(jnp.bfloat16)

    def norm(first, count):
        @pl.loop(0, count // 16)
        def _(i):
            rows = pl.ds(first + i * 16, 16)
            wide = tok_v[rows, :].astype(jnp.float32)
            mean = jnp.mean(wide * wide, axis=-1, keepdims=True)
            tok[me, rows, 0:features] = (wide * lax.rsqrt(mean + EPS)).astype(jnp.bfloat16)

    with scope("norm"):
        loads[3].wait()
        norm(tp * share, share)

    with scope("barrier"):
        pl.semaphore_wait(barrier, groups + ranks - 2)

    with scope("launch"):
        tok_moves(0, start)
        loads[4].wait()
        cast(st_g, sb_g, True, 0)

        if_edge(lambda: starts(0, 0, (6, 7, 4, 5)))
        close_start(0, 0)
        for o in range(1, ranks):
            norm(flip(tp, o, ranks) * share, share)
        loads[5].wait()
        cast(st_u, sb_u, True, 0)
    with scope("near_tokens"):
        tok_arrive(near)
        tok_moves(1, start)

        if_inner(lambda: starts(0, 0, (4, 5, 6, 7)))
        far_start(1, 0)
        close_start(1, 0)
    with scope("casts"):
        for i in range(6, 10):
            loads[i].wait()
        sh[me, 0] = (sg_v[...] * gain_b[...]).astype(jnp.bfloat16)
        sh[me, 1] = (su_v[...] * gain_b[...]).astype(jnp.bfloat16)
        sh[me, 2, 0:rows_d] = sd_v[:, 0:hw].astype(jnp.bfloat16)
        sh[me, 2, rows_d : 2 * rows_d] = sd_v[:, hw:dcols].astype(jnp.bfloat16)
        for piece in range(1, per):
            cast(st_g, sb_g, True, piece)
            cast(st_u, sb_u, True, piece)
        for piece in range(per):
            cast(st_d, sb_d, False, piece)
        for index in range(2):
            for piece in range(per):
                a2a_own(index, piece)
        for piece in range(len(parts)):
            a2a_own(2, piece)
    with scope("far_tokens0"):
        tok_arrive(far[0])
        tok_moves(2, start)
    with scope("far_tokens1"):
        tok_arrive(far[1])
        tok_moves(3, start)
    with scope("side_tokens"):
        for m in (1, 3, 5, 7):
            tok_arrive(flip(me, m, groups))
    with scope("arrive_g0"):
        a2a_arrive(0, 0)
        for part in range(3):
            if_edge(lambda: sh_copy(0, me, part).start())
        a2a_start(0, 1)
    with scope("shares"):
        for o in range(1, groups):
            tok_share(1, flip(me, o, groups)).wait_recv()
            tok_share(2, flip(me, o, groups)).start()
        for i in range(2):
            settle(tok.at[pl.ds(0, groups - 1), mine], tok_trecv.at[i])

    def far_shared(k, part):
        sh_copy(0, far[k], part).wait_recv()
        if_inner(lambda: sh_copy(0, far[k], part).start())
        sh_copy(1, far[k], part).start()

    def near_shared():
        for part in range(3):
            sh_copy(0, near, part).wait_recv()
            if part < 2:
                if_inner(lambda: sh_copy(2, near, part).start())
            sh_copy(1, near, part).start()

    def far_shared_start(part):
        for block in (me, near):
            if_inner(lambda: sh_copy(2, block, part).start())

    def shared_sum(part, blocks):
        total = jnp.zeros((tok_count, hcols), jnp.float32)
        for block in blocks:
            columns = pl.ds(pl.multiple_of(block * rows_w, rows_w), rows_w)
            total = total + jnp.dot(
                tok[me, :, columns], sh[block, part], preferred_element_type=jnp.float32
            )
        return total

    def shid_copy(o):
        return tp_copy(
            shid.at[tp], shid.at[tp], shid_send, shid_recv, flip(tp, o, ranks)
        )

    def hid_core(e, block):
        return tp_copy(
            hid.at[tp, block, e],
            hid.at[tp, block, e],
            hid_send.at[0],
            hid_recv,
            partner,
        )

    def hid_across(e, block):
        return tp_copy(
            hid.at[tp, block, e],
            hid.at[tp, block, e],
            hid_send.at[1],
            hid_yrecv.at[e, block],
            across,
        )

    def hid_forward(e, block):
        return tp_copy(
            hid.at[across, block, e],
            hid.at[across, block, e],
            hid_send.at[2],
            hid_recv,
            partner,
        )

    def turn(o):
        return (me + o) % groups

    for e in range(per):
        with scope(f"arrive_u{e}"):
            if e == 1:

                @pl.when(edge)
                def _():
                    a2a_arrive(0, 1)
                    starts(2, 0, (6, 7, 4, 5))

                close_start(2, 0)
            a2a_arrive(1, e)
            if e == 0:
                a2a_start(1, 1)
                for part in range(3):
                    if_inner(lambda: sh_copy(0, me, part).start())
                    sh_copy(1, me, part).start()
                for part in range(2):
                    if_inner(lambda: sh_copy(2, me, part).start())
            else:
                a2a_start(2, 1)
                far_shared_start(2)
                a2a_start(2, 2)
        with scope(f"hidden{e}"):

            @pl.loop(0, groups)
            def _(o):
                block = turn(o + 1)
                rows = tok[block, :, 0:features]
                first = jnp.dot(rows, rv_g[e], preferred_element_type=jnp.float32)
                second = jnp.dot(rows, rv_u[e], preferred_element_type=jnp.float32)
                hid[tp, block, e] = (jax.nn.silu(first) * second).astype(jnp.bfloat16)

                @pl.when(o >= 1)
                def _():
                    before = turn(o)
                    hid_across(e, before).start()
                    hid_core(e, before).start()

            hid_across(e, me).start()
            hid_core(e, me).start()
        if e == 0:
            with scope("near_shared"):
                if_inner(lambda: near_shared())
        with scope(f"forward{e}"):

            @pl.loop(0, groups)
            def _(o):
                block = turn(o + 1)
                hid_across(e, block).wait_recv()
                hid_forward(e, block).start()

        if e == 0:
            with scope("edge_near_shared"):
                if_edge(lambda: near_shared())
            with scope("far_shared_gu"):
                for k, part in ((0, 0), (0, 1), (1, 0)):
                    far_shared(k, part)

                @pl.when(inner)
                def _():
                    a2a_arrive(0, 1)
                    starts(2, 0, (4, 5, 6, 7))

                far_shared(1, 1)

    with scope("hid_wait"):
        settle(hid.at[pl.ds(0, 2)], hid_recv)
        for kind in range(3):
            settle(hid.at[tp], hid_send.at[kind])

    lanes = lax.broadcasted_iota(jnp.int32, (tok_count, LANES), 1)

    def block_out(block, part):
        offset, wide = parts[part]
        table = tok[block, :, features : features + LANES].astype(jnp.float32)
        total = jnp.zeros((tok_count, wide), jnp.float32)
        for e in range(per):
            expert = me * per + e
            weight = jnp.sum(
                jnp.where(
                    (lanes == expert) | (lanes == expert + experts) | (lanes == expert + 2 * experts),
                    table,
                    0.0,
                ),
                axis=1,
                keepdims=True,
            )
            out = jnp.zeros((tok_count, wide), jnp.float32)
            for r in range(ranks):
                out = out + jnp.dot(
                    hid[r, block, e],
                    rv_d[e, r * hcols : (r + 1) * hcols, offset : offset + wide],
                    preferred_element_type=jnp.float32,
                )
            total = total + weight * out
        return total

    def dest(k):
        half = z // 2
        away = 1 - k // 2
        chosen = half * (1 - away) + (1 - half) * away
        own = (1 - k % 2) * (1 - inn) + (k % 2) * inn
        is_inner = (1 - k % 2) * away + own * (1 - away)
        return chosen * (3 - is_inner) + (1 - chosen) * is_inner

    def x_copy(part, k):
        columns = pl.ds(*parts[part])
        return fs_copy(
            xs.at[k, :, columns], xr.at[k, :, columns], x_send, x_recv.at[part, k], side
        )

    def z_copy(part, k, slot, target, joins=False):
        columns = pl.ds(*parts[part])
        return fs_copy(
            zs.at[k, :, columns],
            zr.at[slot, :, columns],
            z_send,
            z_recv.at[part, slot - 2] if joins else z_last,
            target,
        )

    def x_stage(part, pending):
        columns = pl.ds(*parts[part])

        @pl.loop(0, 4)
        def _(k):
            xs[k, :, columns] = block_out(dest(k) * nx + 1 - x, part).astype(jnp.bfloat16)

            if pending is not None:

                @pl.when(k == 0)
                def _():
                    x_copy(pending, 3).start()

            @pl.when(k >= 1)
            def _():
                x_copy(part, k - 1).start()

    def z_stage(part, pending, low, high, deferred):
        columns = pl.ds(*parts[part])

        @pl.loop(low, high)
        def _(k):
            total = block_out(dest(k) * nx + x, part)

            if pending is not None:

                @pl.when((k == 0) & inner if part == 2 else k == 0)
                def _():
                    x_copy(pending, 3).start()

            @pl.when((k >= 1) & (k < 3) & edge)
            def _():
                z_copy(part, k - 1, k + 1, near, True).start()

            @pl.when(k == 3)
            def _():
                z_copy(part, 2, 4, near).start()

            if deferred:

                @pl.when((k == 2) & inner)
                def _():
                    z_copy(part, 1, 5, far_out).start()

            x_copy(part, k).wait_recv()
            total = total + xr[k, :, columns].astype(jnp.float32)
            acc[k, :, columns] = total
            zs[k, :, columns] = total.astype(jnp.bfloat16)

        if high == 4:
            own_out[:, columns] = acc[3, :, columns]

    def z_join(part, deferred):
        columns = pl.ds(*parts[part])

        @pl.when(inner)
        def _():
            for k in range(2):
                z_copy(part, k, k + 2, near, True).wait_recv()
                zs[k, :, columns] = (
                    acc[k, :, columns] + zr[k + 2, :, columns].astype(jnp.float32)
                ).astype(jnp.bfloat16)
            z_copy(part, 0, 5, far_in).start()
            if not deferred:
                z_copy(part, 1, 5, far_out).start()

    def far_shared_d():
        for k in range(2):
            far_shared(k, 2)

    def x_phase(part, pending):
        with scope(f"arrive_d{part}"):
            a2a_arrive(2, part)
        with scope(f"x_stage{part}"):
            x_stage(part, pending)

    def z_phase(part, pending, low=0, high=4, deferred=False):
        with scope(f"z_stage{part}_{low}"):
            z_stage(part, pending, low, high, deferred)

    def join_phase(part, deferred=False):
        with scope(f"z_join{part}"):
            z_join(part, deferred)

    x_phase(0, None)
    x_phase(1, 0)
    z_phase(0, 1)
    with scope("side_shared_gu"):
        settle(sh.at[pl.ds(0, 4), pl.ds(0, 2)], sh_srecv.at[0])
    with scope("shared_hidden"):
        first, second = (shared_sum(part, range(groups)) for part in range(2))
        shid[tp] = (jax.nn.silu(first) * second).astype(jnp.bfloat16)
        if_inner(lambda: settle(tok.at[pl.ds(0, 3), mine], tok_send.at[0]))
        if_edge(lambda: settle(tok.at[pl.ds(0, 1), mine], tok_send.at[0]))
        settle(tok.at[pl.ds(0, 4), mine], tok_send.at[1])
        if_inner(lambda: settle(tok.at[pl.ds(0, 2), mine], tok_send.at[2]))
        for kind in range(3):
            settle(tok.at[pl.ds(0, groups - 1), mine], tok_tsend.at[kind])
        for o in range(1, ranks):
            shid_copy(o).start()
    with scope("inner_far_shared_d"):
        if_inner(lambda: far_shared_d())
    z_phase(1, None)
    with scope("arrive_d2"):
        a2a_arrive(2, 2)
    join_phase(0)
    with scope("x_stage2"):
        x_stage(2, None)
    join_phase(1)
    with scope("edge_far_shared_d0"):

        @pl.when(edge)
        def _():
            sh_copy(0, far[0], 2).wait_recv()
            x_copy(2, 3).start()
            sh_copy(1, far[0], 2).start()

    z_phase(2, 2, 0, 2)
    with scope("edge_far_shared_d1"):
        if_edge(lambda: far_shared(1, 2))
    join_phase(2, True)
    z_phase(2, None, 2, 4, True)
    with scope("side_shared_d"):
        settle(sh.at[pl.ds(0, 4), 2], sh_srecv.at[1])
    with scope("drain"):
        for index, sent in enumerate((sb_g, sb_u, sb_d)):
            settle(sent.at[pl.ds(0, experts - per)], a2a_send.at[index])
        if_inner(lambda: settle(sh.at[pl.ds(0, 3)], sh_send.at[0]))
        if_edge(lambda: settle(sh.at[pl.ds(0, 1)], sh_send.at[0]))
        settle(sh.at[pl.ds(0, 4)], sh_send.at[1])
        if_inner(lambda: settle(sh.at[pl.ds(0, 2)], sh_send.at[2]))
        settle(xs, x_send)
        settle(zs.at[pl.ds(0, 3)], z_send)
    with scope("last"):
        settle(zr.at[pl.ds(4, 2)], z_last)
        settle(shid.at[pl.ds(0, ranks - 1)], shid_recv)
        settle(shid.at[pl.ds(0, ranks - 1)], shid_send)


def finish_kernel(
    rv_g, rv_u, rv_d, sh, shid, own_out, zr, gate, up, down, sgate, sup, sdown, mixed, mixed_v, sems
):
    rows_d, hw = sdown.shape[1], sdown.shape[2] // 2
    groups, hcols = sh.shape[0], shid.shape[2]
    moves = [
        (rv_g, gate),
        (rv_u, up),
        (rv_d, down),
        (sh.at[:, 0], sgate),
        (sh.at[:, 1], sup),
        (sh.at[:, 2, pl.ds(0, rows_d)], sdown.at[:, :, pl.ds(0, hw)]),
        (sh.at[:, 2, pl.ds(rows_d, rows_d)], sdown.at[:, :, pl.ds(hw, hw)]),
    ]
    copies = [pltpu.make_async_copy(a, b, sems.at[i]) for i, (a, b) in enumerate(moves)]
    for copy in copies:
        copy.start()
    for part in range(2):
        columns = slice(part * hw, (part + 1) * hw)
        total = own_out[:, columns]
        for slot in (4, 5):
            total = total + zr[slot, :, columns].astype(jnp.float32)
        for block in range(groups):
            at = block * rows_d
            total = total + jnp.dot(
                shid[at // hcols, :, at % hcols : at % hcols + rows_d],
                sh[block, 2, part * rows_d : (part + 1) * rows_d],
                preferred_element_type=jnp.float32,
            )
        mixed_v[:, columns] = total.astype(jnp.bfloat16)
    last = pltpu.make_async_copy(mixed_v, mixed, sems.at[len(moves)])
    last.start()
    for copy in copies:
        copy.wait()
    last.wait()


def dense_body(
    tokens,
    norm_gain,
    expert_gate,
    expert_up,
    expert_down,
    shared_gate,
    shared_up,
    shared_down,
    expert_ids,
    route_weights,
):
    groups, ranks = lax.axis_size("fs"), lax.axis_size("tp")
    experts, rows_w, hcols = expert_gate.shape
    rows_d, dcols = expert_down.shape[1:]
    per = experts // groups
    tok_count, features = tokens.shape
    total = features + LANES
    bf, f32 = jnp.bfloat16, jnp.float32
    dma = pltpu.SemaphoreType.DMA
    any_space = pl.BlockSpec(memory_space=pl.ANY)
    vmem = pl.BlockSpec(memory_space=pltpu.VMEM)
    hidden = hcols * ranks
    wide_rows = -(-tok_count // LANES) * LANES
    made = pl.pallas_call(
        functools.partial(fused_kernel, groups, ranks),
        out_shape=(
            pltpu.VMEM((per, features, hcols), bf),
            pltpu.VMEM((per, features, hcols), bf),
            pltpu.VMEM((per, hidden, dcols), bf),
            pltpu.VMEM((groups, 3, rows_w, hcols), bf),
            pltpu.VMEM((ranks, tok_count, hcols), bf),
            pltpu.VMEM((tok_count, dcols), f32),
            pltpu.VMEM((6, tok_count, dcols), bf),
        ),
        in_specs=[any_space] * 10,
        out_specs=(vmem,) * 7,
        scratch_shapes=[
            pltpu.VMEM((tok_count, features), bf),
            pltpu.VMEM((1, rows_w), f32),
            pltpu.VMEM((TOP_K, tok_count), jnp.int32),
            pltpu.VMEM((TOP_K, tok_count), f32),
            pltpu.VMEM((rows_w, hcols), f32),
            pltpu.VMEM((rows_w, hcols), f32),
            pltpu.VMEM((rows_d, dcols), f32),
            pltpu.VMEM((rows_w, hcols), f32),
            pltpu.VMEM((LANES, wide_rows), f32),
            pltpu.VMEM((experts, rows_w, hcols), f32),
            pltpu.VMEM((experts, rows_w, hcols), f32),
            pltpu.VMEM((experts, rows_d, dcols), f32),
            pltpu.VMEM((experts, rows_w, hcols), bf),
            pltpu.VMEM((experts, rows_w, hcols), bf),
            pltpu.VMEM((experts, rows_d, dcols), bf),
            pltpu.VMEM((groups, tok_count, total), bf),
            pltpu.VMEM((ranks, groups, per, tok_count, hcols), bf),
            pltpu.VMEM((4, tok_count, dcols), bf),
            pltpu.VMEM((4, tok_count, dcols), bf),
            pltpu.VMEM((4, tok_count, dcols), bf),
            pltpu.VMEM((4, tok_count, dcols), f32),
            dma((10,)),
            dma((3,)),
            dma((3, max(per, 3))),
            dma((3,)),
            dma((groups,)),
            dma((3,)),
            dma((2,)),
            dma((groups,)),
            dma((3,)),
            dma((groups // 2, 3)),
            dma((2,)),
            dma((3,)),
            dma,
            dma((per, groups)),
            dma,
            dma,
            dma,
            dma((3, 4)),
            dma,
            dma((3, 2)),
            dma,
        ],
        compiler_params=pltpu.CompilerParams(
            collective_id=0, has_side_effects=True, vmem_limit_bytes=VMEM_BYTES
        ),
    )(
        tokens,
        norm_gain[None, :],
        expert_ids.T,
        route_weights.T,
        expert_gate,
        expert_up,
        expert_down,
        shared_gate,
        shared_up,
        shared_down,
    )
    gate, up, down, sgate, sup, sdown, mixed = pl.pallas_call(
        finish_kernel,
        out_shape=tuple(
            jax.ShapeDtypeStruct(shape, bf)
            for shape in (
                (per, features, hcols),
                (per, features, hcols),
                (per, hidden, dcols),
                (groups, rows_w, hcols),
                (groups, rows_w, hcols),
                (groups, rows_d, dcols),
                (tok_count, dcols),
            )
        ),
        in_specs=[vmem] * 7,
        out_specs=(any_space,) * 7,
        scratch_shapes=[pltpu.VMEM((tok_count, dcols), bf), dma((8,))],
        compiler_params=pltpu.CompilerParams(vmem_limit_bytes=VMEM_BYTES // 4),
    )(*made)
    return (
        gate,
        up,
        down,
        sgate.reshape(features, hcols),
        sup.reshape(features, hcols),
        sdown.reshape(hidden, dcols),
        mixed,
    )


def expert_hidden(rows, gate_new, up_new):
    first = jnp.einsum("secn,enf->secf", rows, gate_new, preferred_element_type=jnp.float32)
    second = jnp.einsum("secn,enf->secf", rows, up_new, preferred_element_type=jnp.float32)
    return (jax.nn.silu(first) * second).astype(jnp.bfloat16)


def body(
    tokens,
    norm_gain,
    expert_gate,
    expert_up,
    expert_down,
    shared_gate,
    shared_up,
    shared_down,
    expert_ids,
    route_weights,
):
    groups = lax.axis_size("fs")
    experts = expert_gate.shape[0]
    per_group = experts // groups
    tok_count = tokens.shape[0]
    capacity = 2 * tok_count * TOP_K // experts
    ranks = lax.axis_size("tp")
    square = expert_down.shape[1] * expert_down.shape[2] == shared_gate.size
    if capacity >= tok_count and per_group >= 2 and groups == 8 and ranks == 4 and square:
        return dense_body(
            tokens,
            norm_gain,
            expert_gate,
            expert_up,
            expert_down,
            shared_gate,
            shared_up,
            shared_down,
            expert_ids,
            route_weights,
        )
    gate_local = (expert_gate * norm_gain[None, :, None]).astype(jnp.bfloat16)
    up_local = (expert_up * norm_gain[None, :, None]).astype(jnp.bfloat16)
    down_local = expert_down.astype(jnp.bfloat16)
    gate_local = gate_local.reshape((groups, per_group) + gate_local.shape[1:])
    up_local = up_local.reshape((groups, per_group) + up_local.shape[1:])
    down_local = down_local.reshape((groups, per_group) + down_local.shape[1:])
    shared_first_local = (shared_gate * norm_gain[:, None]).astype(jnp.bfloat16)
    shared_second_local = (shared_up * norm_gain[:, None]).astype(jnp.bfloat16)
    shared_third_local = shared_down.astype(jnp.bfloat16)
    gate_moved, up_moved, down_moved = (
        lax.all_to_all(gate_local, "fs", split_axis=0, concat_axis=2, tiled=True),
        lax.all_to_all(up_local, "fs", split_axis=0, concat_axis=2, tiled=True),
        lax.all_to_all(down_local, "fs", split_axis=0, concat_axis=2, tiled=True),
    )
    down_ready = down_moved[0]
    gate_ready = gate_moved[0]
    up_ready = up_moved[0]
    shared_gate_ready, shared_up_ready, shared_down_ready = (
        lax.all_gather(shared_first_local, "fs", axis=0, tiled=True),
        lax.all_gather(shared_second_local, "fs", axis=0, tiled=True),
        lax.all_gather(shared_third_local, "fs", axis=0, tiled=True),
    )
    wide = tokens.astype(jnp.float32)
    normed = (wide * lax.rsqrt(jnp.mean(wide * wide, axis=-1, keepdims=True) + EPS)).astype(
        jnp.bfloat16
    )
    chosen = expert_ids.reshape(-1)
    onehot = (chosen[:, None] == jnp.arange(experts, dtype=jnp.int32)[None, :]).astype(jnp.int32)
    ranks = jnp.sum(jnp.cumsum(onehot, axis=0) * onehot, axis=1) - 1
    owners = jnp.arange(tok_count * TOP_K, dtype=jnp.int32) // TOP_K
    slot_token = jnp.zeros((experts, capacity), jnp.int32).at[chosen, ranks].set(owners)
    outgoing = normed[slot_token.reshape(-1)].reshape(groups, per_group, capacity, normed.shape[1])
    share = capacity // lax.axis_size("tp")
    mine = lax.dynamic_slice_in_dim(outgoing, lax.axis_index("tp") * share, share, 2)
    arrived = lax.all_to_all(mine, "fs", split_axis=0, concat_axis=0, tiled=True)
    hidden = expert_hidden(lax.all_gather(arrived, "tp", axis=2, tiled=True), gate_ready, up_ready)
    shared_first = jnp.dot(normed, shared_gate_ready, preferred_element_type=jnp.float32)
    shared_second = jnp.dot(normed, shared_up_ready, preferred_element_type=jnp.float32)
    shared_hidden = (jax.nn.silu(shared_first) * shared_second).astype(jnp.bfloat16)[None, None]
    columns = down_ready.shape[2]
    routed_piece = lax.all_gather(hidden, "tp", axis=3, tiled=True)
    shared_piece = lax.all_gather(shared_hidden, "tp", axis=3, tiled=True)
    routed_total = jnp.einsum(
        "secf,efd->secd", routed_piece, down_ready, preferred_element_type=jnp.float32
    )
    shared_total = jnp.einsum(
        "abtf,fd->abtd", shared_piece, shared_down_ready, preferred_element_type=jnp.float32
    )
    returned = lax.all_to_all(
        routed_total.astype(jnp.bfloat16), "fs", split_axis=0, concat_axis=0, tiled=True
    )
    returned = returned.reshape(experts * capacity, columns)
    picked = (
        returned[chosen * capacity + ranks].astype(jnp.float32).reshape(tok_count, TOP_K, columns)
    )
    routed = jnp.sum(picked * route_weights[:, :, None], axis=1)
    mixed = (shared_total[0, 0] + routed).astype(jnp.bfloat16)
    return (
        gate_ready,
        up_ready,
        down_ready,
        shared_gate_ready,
        shared_up_ready,
        shared_down_ready,
        mixed,
    )


def solution(mesh):
    in_specs = (
        P("fs", None),
        P("fs"),
        P(None, "fs", "tp"),
        P(None, "fs", "tp"),
        P(None, "fs", "tp"),
        P("fs", "tp"),
        P("fs", "tp"),
        P("fs", "tp"),
        P("fs", None),
        P("fs", None),
    )
    out_specs = (
        P("fs", None, "tp"),
        P("fs", None, "tp"),
        P("fs", None, "tp"),
        P(None, "tp"),
        P(None, "tp"),
        P(None, "tp"),
        P("fs", "tp"),
    )
    return jax.shard_map(body, mesh=mesh, in_specs=in_specs, out_specs=out_specs, check_vma=False)
```
